32 devices in a mesh: sp: 4 (over z), dp: 8 (over y, x, core).
Axes of the slice: x: 2, y: 2, z: 4, core: 2. Of those that a mesh axis runs over, the one named last changes fastest.
Arguments:
- inputs: bfloat16 [8, 544, 2048], P('dp', 'sp'), may hold values from -6 to 6
- query_vectors: bfloat16 [8, 544, 1024], P('dp', 'sp'), may hold values from -6 to 6
- key_vectors: bfloat16 [8, 544, 1024], P('dp', 'sp'), may hold values from -6 to 6
- value_vectors: bfloat16 [8, 544, 1024], P('dp', 'sp'), may hold values from -6 to 6
- cotangent: bfloat16 [8, 544, 1024], P('dp', 'sp'), may hold values from -6 to 6
- gate_prefix: float32 [8, 16, 544], P('dp', 'sp'), may hold values from -544 to 0, as said below
- value_weight: bfloat16 [2048, 1024], P('sp', 'dp'), may hold values from -0.125 to 0.125
Outputs:
- query_grad: bfloat16 [8, 544, 1024], P('dp', 'sp')
- key_grad: bfloat16 [8, 544, 1024], P('dp', 'sp')
- input_grad: bfloat16 [8, 544, 2048], P('dp', 'sp')
- weight_grad: float32 [2048, 1024], P('sp', 'dp')
The draws below stay inside these ranges and needn't reach their ends.
Inputs may be any that keep to these rules, and one draw needn't show every extreme that they name: `gate_prefix`: non-increasing along the positions of each sequence and head.
All inputs are finite; a program needn't handle non-finite values.
Results may differ from the reference program's by a relative error of at most 0.015.
Values may be sent and summed in bfloat16 or wider, within the bound.
A program may use at most 128 MiB of HBM per device.

```python
import jax
import jax.numpy as jnp
from jax import lax

MODEL = 2048
HEADS = 16
HEAD_DIM = 64
TOK_DEV = 136
VALUE_WIDTH = 1024
SEQS = 8
LEN = 544
QBLOCK = 544


def paired_vectors(key):
    folded = jax.random.fold_in(key, 11)
    query_seed, key_seed, spot_seed, sign_seed = jax.random.split(folded, 4)
    shape = (SEQS, LEN, HEADS * HEAD_DIM)
    query_draw = jnp.clip(jax.random.normal(query_seed, shape, jnp.float32), -4.0, 4.0)
    key_draw = jnp.clip(jax.random.normal(key_seed, shape, jnp.float32), -4.0, 4.0)
    return (query_draw, key_draw)


def draw_query_vectors(key, part):
    return paired_vectors(key)[0].astype(jnp.bfloat16)


def draw_key_vectors(key, part):
    return paired_vectors(key)[1].astype(jnp.bfloat16)


def draw_gate_prefix(key, part):
    folded = jax.random.fold_in(key, 23)
    order_seed, fast_seed, slow_seed, step_seed, span_seed = jax.random.split(folded, 5)
    head_order = jax.random.permutation(order_seed, HEADS)
    fast_count = HEADS // 2
    fast_heads = (head_order < fast_count)[None, :, None]
    fast_rate = jax.random.uniform(fast_seed, (SEQS, HEADS, 1), jnp.float32, 0.05, 0.15)
    slow_rate = jax.random.uniform(slow_seed, (SEQS, HEADS, 1), jnp.float32, 0.25, 0.75) / LEN
    step_rate = jnp.where(fast_heads, fast_rate, slow_rate)
    step_factor = jax.random.uniform(step_seed, (SEQS, HEADS, LEN), jnp.float32, 0.5, 1.5)
    span_factor = jnp.exp(jax.random.uniform(span_seed, (SEQS, HEADS, LEN // TOK_DEV), jnp.float32, -0.6931, 0.6931))
    span_factor = jnp.repeat(span_factor, TOK_DEV, axis=2)
    log_steps = -step_rate * step_factor * span_factor
    return jnp.cumsum(log_steps, axis=2)


def steps_of(key, extent, shards, low, largest):
    loudness = 1.0
    for position, shards_of in shards:
        heights = jax.random.uniform(jax.random.fold_in(jax.random.fold_in(key, 6), position), (shards_of,), jnp.float32, low / len(shards), largest / len(shards))
        loudness = loudness * jnp.repeat(jnp.exp(heights), extent[position] // shards_of).reshape((-1,) + (1,) * (len(extent) - 1 - position))
    return loudness


def noise(rng, dims, spread, limit, shards=(), kind=jnp.bfloat16):
    drawn = jax.random.normal(rng, dims, jnp.float32) * spread
    if len(shards) > 0:
        drawn = steps_of(rng, dims, shards, -0.22, 0.18) * drawn
    return jnp.clip(drawn, min=-limit, max=limit).astype(kind)


def setup_inputs(seed: int = 0) -> dict:
    key_of = jax.random.split(jax.random.key(seed), 8)
    return {
        "inputs": noise(key_of[0], (SEQS, LEN, MODEL), 1.0, 6.0, ((0, 8), (1, 4))),
        "query_vectors": draw_query_vectors(jax.random.fold_in(key_of[7], 71), 0),
        "key_vectors": draw_key_vectors(jax.random.fold_in(key_of[7], 71), 0),
        "value_vectors": noise(key_of[3], (SEQS, LEN, VALUE_WIDTH), 1.0, 6.0, ((0, 8), (1, 4))),
        "cotangent": noise(key_of[4], (SEQS, LEN, VALUE_WIDTH), 1.0, 6.0, ((0, 8), (1, 4))),
        "gate_prefix": draw_gate_prefix(jax.random.fold_in(key_of[7], 71), 0),
        "value_weight": noise(key_of[6], (MODEL, VALUE_WIDTH), MODEL ** -0.5, 0.125, ((0, 4), (1, 8))),
    }


def sequence_backward(query_heads, key_heads, value_heads, grad_heads, prefix):
    score_scale = HEAD_DIM ** -0.5
    query_wide = query_heads.astype(jnp.float32)
    key_wide = key_heads.astype(jnp.float32)
    value_wide = value_heads.astype(jnp.float32)
    grad_wide = grad_heads.astype(jnp.float32)
    key_accum = jnp.zeros(key_wide.shape, jnp.float32)
    value_accum = jnp.zeros(key_wide.shape, jnp.float32)
    query_parts = []
    for block_index in range(LEN // QBLOCK):
        first_row = block_index * QBLOCK
        last_row = first_row + QBLOCK
        query_rows = query_wide[first_row:last_row]
        key_rows = key_wide[:last_row]
        grad_rows = grad_wide[first_row:last_row]
        scores = jnp.einsum('qhd,khd->hqk', query_rows, key_rows) * score_scale
        scores = scores + prefix[:, first_row:last_row, None] - prefix[:, None, :last_row]
        causal = jnp.arange(last_row)[None, :] <= (first_row + jnp.arange(QBLOCK))[:, None]
        scores = jnp.where(causal[None], scores, -jnp.inf)
        row_peak = jnp.max(scores, axis=-1, keepdims=True)
        raised_scores = jnp.exp(scores - row_peak)
        softmax_rows = raised_scores / jnp.sum(raised_scores, axis=-1, keepdims=True)
        softmax_low = lax.optimization_barrier(softmax_rows.astype(jnp.bfloat16)).astype(jnp.float32)
        value_accum = value_accum.at[:last_row].add(jnp.einsum('hqk,qhd->khd', softmax_low, grad_rows))
        softmax_grad = jnp.einsum('qhd,khd->hqk', grad_rows, value_wide[:last_row])
        row_term = jnp.sum(softmax_rows * softmax_grad, axis=-1, keepdims=True)
        score_grad = softmax_rows * (softmax_grad - row_term)
        score_low = lax.optimization_barrier(score_grad.astype(jnp.bfloat16)).astype(jnp.float32)
        query_parts.append((jnp.einsum('hqk,khd->qhd', score_low, key_rows) * score_scale).astype(jnp.bfloat16))
        key_accum = key_accum.at[:last_row].add(jnp.einsum('hqk,qhd->khd', score_low, query_rows))
    query_grad = jnp.concatenate(query_parts, axis=0)
    key_grad = (key_accum * score_scale).astype(jnp.bfloat16)
    return query_grad, key_grad, value_accum.astype(jnp.bfloat16)


def reference(inputs, query_vectors, key_vectors, value_vectors, cotangent, gate_prefix, value_weight):
    head_shape = (LEN, HEADS, HEAD_DIM)

    def per_sequence(weight_total, sequence_items):
        seq_inputs, seq_query, seq_key, seq_value, seq_grad, seq_prefix = sequence_items
        query_grad, key_grad, value_grad = sequence_backward(
            seq_query.reshape(head_shape), seq_key.reshape(head_shape),
            seq_value.reshape(head_shape), seq_grad.reshape(head_shape), seq_prefix)
        value_flat = value_grad.reshape(LEN, VALUE_WIDTH)
        input_grad = jnp.dot(value_flat, value_weight.T, preferred_element_type=jnp.float32).astype(jnp.bfloat16)
        weight_total = weight_total + jnp.dot(seq_inputs.T, value_flat, preferred_element_type=jnp.float32)
        return weight_total, (query_grad.reshape(LEN, VALUE_WIDTH), key_grad.reshape(LEN, VALUE_WIDTH), input_grad)

    weight_total, outputs = lax.scan(
        per_sequence, jnp.zeros((MODEL, VALUE_WIDTH), jnp.float32),
        (inputs, query_vectors, key_vectors, value_vectors, cotangent, gate_prefix))
    query_grad, key_grad, input_grad = outputs
    return (query_grad, key_grad, input_grad, weight_total)
```

```python
import functools

import jax
import jax.numpy as jnp
from jax import lax
from jax.experimental import pallas as pl
from jax.experimental.pallas import tpu as pltpu
from jax.sharding import PartitionSpec as P

HEAD_DIM = 64


def attention_backward(query_heads, key_heads, value_heads, grad_heads, prefix):
    length = query_heads.shape[0]
    score_scale = HEAD_DIM ** (-0.5)
    block_count = max(1, length // 512)
    block_rows = length // block_count
    key_accum = jnp.zeros(key_heads.shape, jnp.float32)
    value_accum = jnp.zeros(key_heads.shape, jnp.float32)
    query_parts = []
    for block_index in range(block_count):
        first_row = block_index * block_rows
        last_row = first_row + block_rows
        query_rows = query_heads[first_row:last_row]
        key_rows = key_heads[:last_row]
        grad_rows = grad_heads[first_row:last_row]
        scores = (
            jnp.einsum("qhd,khd->hqk", query_rows, key_rows, preferred_element_type=jnp.float32)
            * score_scale
        )
        scores = scores + prefix[:, first_row:last_row, None] - prefix[:, None, :last_row]
        causal = jnp.arange(last_row)[None, :] <= (first_row + jnp.arange(block_rows))[:, None]
        scores = jnp.where(causal[None], scores, -jnp.inf)
        row_peak = jnp.max(scores, axis=-1, keepdims=True)
        raised_scores = jnp.exp(scores - row_peak)
        softmax_rows = raised_scores / jnp.sum(raised_scores, axis=-1, keepdims=True)
        softmax_low = softmax_rows.astype(jnp.bfloat16)
        value_accum = value_accum.at[:last_row].add(
            jnp.einsum("hqk,qhd->khd", softmax_low, grad_rows, preferred_element_type=jnp.float32)
        )
        softmax_grad = jnp.einsum(
            "qhd,khd->hqk", grad_rows, value_heads[:last_row], preferred_element_type=jnp.float32
        )
        row_term = jnp.sum(softmax_rows * softmax_grad, axis=-1, keepdims=True)
        score_low = (softmax_rows * (softmax_grad - row_term)).astype(jnp.bfloat16)
        query_parts.append(
            (
                jnp.einsum("hqk,khd->qhd", score_low, key_rows, preferred_element_type=jnp.float32)
                * score_scale
            ).astype(jnp.bfloat16)
        )
        key_accum = key_accum.at[:last_row].add(
            jnp.einsum("hqk,qhd->khd", score_low, query_rows, preferred_element_type=jnp.float32)
        )
    query_grad = jnp.concatenate(query_parts, axis=0)
    key_grad = (key_accum * score_scale).astype(jnp.bfloat16)
    return (query_grad, key_grad, value_accum.astype(jnp.bfloat16))


def shards(inputs, query_vectors, key_vectors, value_vectors, cotangent, gate_prefix, value_weight):
    query_seq, key_seq, value_seq, grad_seq, input_cols = (
        lax.all_to_all(query_vectors[0], "sp", split_axis=1, concat_axis=0, tiled=True),
        lax.all_to_all(key_vectors[0], "sp", split_axis=1, concat_axis=0, tiled=True),
        lax.all_to_all(value_vectors[0], "sp", split_axis=1, concat_axis=0, tiled=True),
        lax.all_to_all(cotangent[0], "sp", split_axis=1, concat_axis=0, tiled=True),
        lax.all_to_all(inputs[0], "sp", split_axis=1, concat_axis=0, tiled=True),
    )
    length = query_seq.shape[0]
    local_width = query_seq.shape[1]
    head_shape = (length, local_width // HEAD_DIM, HEAD_DIM)
    query_heads, key_heads, value_heads = attention_backward(
        query_seq.reshape(head_shape),
        key_seq.reshape(head_shape),
        value_seq.reshape(head_shape),
        grad_seq.reshape(head_shape),
        gate_prefix[0],
    )
    query_flat = query_heads.reshape(length, local_width)
    key_flat = key_heads.reshape(length, local_width)
    value_flat = value_heads.reshape(length, local_width)
    value_all = lax.all_gather(value_flat, "sp", axis=1, tiled=True)
    weight_block = lax.all_gather(value_weight, "dp", axis=1, tiled=True)
    weight_rows = lax.psum_scatter(
        lax.dot_general(
            value_all, input_cols, (((0,), (0,)), ((), ())), preferred_element_type=jnp.float32
        ).astype(jnp.bfloat16),
        "dp",
        scatter_dimension=0,
        tiled=True,
    ).astype(jnp.float32)
    weight_grad = weight_rows.T
    query_back, key_back = (
        lax.all_to_all(query_flat, "sp", split_axis=0, concat_axis=1, tiled=True),
        lax.all_to_all(key_flat, "sp", split_axis=0, concat_axis=1, tiled=True),
    )
    column_grad = lax.dot_general(
        value_all, weight_block, (((1,), (1,)), ((), ())), preferred_element_type=jnp.float32
    ).astype(jnp.bfloat16)
    input_grad = lax.all_to_all(column_grad, "sp", split_axis=0, concat_axis=1, tiled=True)
    return (query_back[None], key_back[None], input_grad[None], weight_grad)


LANES = 128
MESH = pl.DeviceIdType.MESH


def one_kernel_fits(sp_count, dp_count, inputs, query, key, value, cotangent, gate, weight):
    rows, width = query.shape[1:]
    model = inputs.shape[2]
    return (
        dp_count == 8
        and width == dp_count * LANES
        and width % (sp_count * LANES) == 0
        and LANES == 2 * HEAD_DIM
        and rows % 8 == 0
        and model % (sp_count * LANES) == 0
        and model % (2 * LANES) == 0
        and sp_count % 2 == 0
        and rows * sp_count <= 1024
        and (dp_count * rows + width) * model <= 3 * 2**21
    )


def attention_pair(q32, k32, v32, g32, rows_of, columns_of, stats):
    length = q32.shape[0]
    scale = HEAD_DIM ** (-0.5)
    dot = functools.partial(lax.dot_general, preferred_element_type=jnp.float32)
    dq_ref, dk_ref, dv_ref = stats
    lane = lax.broadcasted_iota(jnp.int32, (length, LANES), 1)
    q_all = q32.astype(jnp.bfloat16)
    g_all = g32.astype(jnp.bfloat16)
    for head in range(2):
        own = (lane < HEAD_DIM) if head == 0 else (lane >= HEAD_DIM)
        q_own, k_own, v_own, g_own = (
            jnp.where(own, x, 0.0).astype(jnp.bfloat16) for x in (q32, k32, v32, g32)
        )
        gate_row, gate_column = rows_of[head], columns_of[head]
        first = 0
        while first < length:
            last = min(first + 256, length)
            size = last - first
            scores = dot(k_own[:last], q_all[first:last], (((1,), (1,)), ((), ()))) * scale
            scores = scores + gate_row[:, first:last] - gate_column[:last]
            key_pos = lax.broadcasted_iota(jnp.int32, (last, size), 0)
            query_pos = lax.broadcasted_iota(jnp.int32, (last, size), 1) + first
            scores = jnp.where(key_pos <= query_pos, scores, -jnp.inf)
            peak = jnp.max(scores, axis=0, keepdims=True)
            raised = jnp.exp(scores - peak)
            soft = raised * (1.0 / jnp.sum(raised, axis=0, keepdims=True))
            soft_grad = dot(v_own[:last], g_all[first:last], (((1,), (1,)), ((), ())))
            row_term = jnp.sum(soft * soft_grad, axis=0, keepdims=True)
            score_low = (soft * (soft_grad - row_term)).astype(jnp.bfloat16)
            dv = dot(soft.astype(jnp.bfloat16), g_own[first:last], (((1,), (0,)), ((), ())))
            dk = dot(score_low, q_own[first:last], (((1,), (0,)), ((), ()))) * scale
            dq = dot(score_low, k_own[:last], (((0,), (0,)), ((), ()))) * scale
            seen = first if head == 0 else last
            if seen:
                dv_ref[:seen] += dv[:seen]
                dk_ref[:seen] += dk[:seen]
            if seen < last:
                dv_ref[seen:last] = dv[seen:]
                dk_ref[seen:last] = dk[seen:]
            if head == 0:
                dq_ref[first:last] = dq
            else:
                dq_ref[first:last] += dq
            first = last


def kernel(
    n, groups, in_ref, q_ref, k_ref, v_ref, g_ref, gate_ref, w_ref,
    qg_ref, kg_ref, ig_ref, wg_ref,
    pair_in, pair_out, vg, vg_seq, x_all, w_all, part, part_in, gate_pad, gate_t,
    dq_ref, dk_ref, dv_ref, send_sems, recv_sems,
):
    s = lax.axis_index("sp")
    d = lax.axis_index("dp")
    core, x, y = d % 2, (d // 2) % 2, d // 4
    rows = q_ref.shape[0]
    length = n * rows
    half = in_ref.shape[1] // 2

    def near(step):
        return (
            d
            + (step % 2) * (1 - 2 * core)
            + ((step // 2) % 2) * (2 - 4 * x)
            + (step // 4) * (4 - 8 * y)
        )

    partner, x_near, y_near, corner = near(1), near(2), near(4), near(6)
    started = []

    def send(src, dst, to_sp, to_dp):
        index = len(started)
        copy = pltpu.make_async_remote_copy(
            src_ref=src,
            dst_ref=dst,
            send_sem=send_sems.at[index],
            recv_sem=recv_sems.at[index],
            device_id={"sp": to_sp, "dp": to_dp},
            device_id_type=MESH,
        )
        copy.start()
        started.append(copy)
        return copy

    barrier = pltpu.get_barrier_semaphore()
    for r in range(1, n):
        pl.semaphore_signal(barrier, inc=1, device_id={"sp": (s + r) % n, "dp": d}, device_id_type=MESH)
    for step in range(1, 8):
        pl.semaphore_signal(barrier, inc=1, device_id={"sp": s, "dp": near(step)}, device_id_type=MESH)
    pl.semaphore_wait(barrier, n - 1 + 7)

    arrived = []
    for p in range(groups):
        for a, ref in enumerate((q_ref, k_ref, v_ref, g_ref)):
            for r in range(1, n):
                to = (s + r) % n
                columns = pl.ds(pl.multiple_of((to * groups + p) * LANES, LANES), LANES)
                arrived.append(send(ref.at[:, columns], pair_in.at[p, a, s], to, d))
    x_near0 = send(in_ref, x_all.at[d], s, x_near)
    y_near0 = send(in_ref, x_all.at[d], s, y_near)
    x_part0 = send(in_ref, x_all.at[d], s, partner)
    w_came = [send(w_ref, w_all.at[d, s], (s + r) % n, d) for r in range(1, n)]

    for p in range(groups):
        columns = pl.ds(pl.multiple_of((s * groups + p) * LANES, LANES), LANES)
        for a, ref in enumerate((q_ref, k_ref, v_ref, g_ref)):
            pair_in[p, a, s] = ref[:, columns]
    x_all[d] = in_ref[...]
    w_all[d, s] = w_ref[...]
    gate_pad[...] = jnp.zeros_like(gate_pad)
    gate_pad[: gate_ref.shape[0], :length] = gate_ref[...]
    gate_t[...] = gate_pad[...].T

    back_v, back_qk = [], []

    def attend(p):
        for copy in arrived[p * 4 * (n - 1) : (p + 1) * 4 * (n - 1)]:
            copy.wait_recv()
        wide = [pair_in[p, a].astype(jnp.float32).reshape(length, LANES) for a in range(4)]
        heads = (2 * p, 2 * p + 1)
        attention_pair(
            *wide,
            [gate_pad[h : h + 1, :length] for h in heads],
            [gate_t[:length, h : h + 1] for h in heads],
            (dq_ref, dk_ref, dv_ref),
        )
        for a, ref in enumerate((dv_ref, dq_ref, dk_ref)):
            pair_out[p, a] = ref[...].reshape(n, rows, LANES).astype(jnp.bfloat16)
        columns = pl.ds(pl.multiple_of((s * groups + p) * LANES, LANES), LANES)
        for a, ref in enumerate((None, qg_ref, kg_ref)):
            for r in range(1, n):
                to = (s + r) % n
                if a == 0:
                    back_v.append(send(pair_out.at[p, a, to], vg.at[s * groups + p], to, d))
                else:
                    back_qk.append(send(pair_out.at[p, a, to], ref.at[:, columns], to, d))
            if a == 0:
                vg[s * groups + p] = pair_out[p, a, s]
            else:
                ref[:, columns] = pair_out[p, a, s]

    def spread_middle(buffer, low, high, from_x, from_y):
        from_x.wait_recv()
        a = send(low(x_near), low(x_near), s, y_near)
        b = send(buffer.at[x_near], buffer.at[x_near], s, partner)
        from_y.wait_recv()
        c = send(high(y_near), high(y_near), s, x_near)
        e = send(buffer.at[y_near], buffer.at[y_near], s, partner)
        return a, c, b, e

    def spread_last(buffer, middle):
        middle[0].wait_recv()
        middle[1].wait_recv()
        return send(buffer.at[corner], buffer.at[corner], s, partner)

    x_low = lambda i: x_all.at[i, :, pl.ds(0, half)]
    x_high = lambda i: x_all.at[i, :, pl.ds(half, half)]
    w_low = lambda i: w_all.at[i, pl.ds(0, n // 2)]
    w_high = lambda i: w_all.at[i, pl.ds(n // 2, n // 2)]

    x_middle = x_last = None
    for p in range(groups):
        attend(p)
        if p == 0:
            x_middle = spread_middle(x_all, x_low, x_high, x_near0, y_near0)
    x_last = spread_last(x_all, x_middle)

    for copy in w_came:
        copy.wait_recv()
    w_x = send(w_all.at[d], w_all.at[d], s, x_near)
    w_y = send(w_all.at[d], w_all.at[d], s, y_near)
    w_part = send(w_all.at[d], w_all.at[d], s, partner)

    for copy in back_v:
        copy.wait_recv()
    moved = [send(vg.at[near(step)], vg_seq.at[d], s, near(step)) for step in range(1, 8)]
    vg_seq[d] = vg[d]
    for copy in moved:
        copy.wait_recv()
    for copy in (x_part0, x_middle[2], x_middle[3], x_last):
        copy.wait_recv()

    block = in_ref.shape[1] // n
    dot = functools.partial(lax.dot_general, preferred_element_type=jnp.float32)
    for j in range(n):
        total = None
        for i in range(8):
            term = dot(vg_seq[i], x_all[i, :, j * block : (j + 1) * block], (((0,), (0,)), ((), ())))
            total = term if total is None else total + term
        part[j] = total.astype(jnp.bfloat16)
    sums = [send(part.at[(s + r) % n], part_in.at[r - 1], (s + r) % n, d) for r in range(1, n)]

    w_middle = spread_middle(w_all, w_low, w_high, w_x, w_y)
    w_last = spread_last(w_all, w_middle)
    for copy in (w_part, w_middle[2], w_middle[3], w_last):
        copy.wait_recv()
    vg_rows = jnp.concatenate([vg[i] for i in range(8)], axis=1)
    for j in range(n):
        w_rows = jnp.concatenate([w_all[i, j] for i in range(8)], axis=1)
        ig_ref[:, j * block : (j + 1) * block] = dot(
            vg_rows, w_rows, (((1,), (1,)), ((), ()))
        ).astype(jnp.bfloat16)

    total = part[s].astype(jnp.float32)
    for r, copy in enumerate(sums):
        copy.wait_recv()
        total = total + part_in[r].astype(jnp.float32)
    wg_ref[...] = total.T
    for copy in back_qk:
        copy.wait_recv()
    for copy in started:
        copy.wait_send()


def fused(mesh, inputs, query, key, value, cotangent, gate, weight):
    n = mesh.shape["sp"]
    rows, width = query.shape[1:]
    model = inputs.shape[2]
    groups = width // (n * LANES)
    length = n * rows
    padded = -(-length // LANES) * LANES
    bf16, f32 = jnp.bfloat16, jnp.float32
    copies = (n - 1) * (4 * groups + 1 + 3 * groups + 1) + 2 * 8 + 7
    vmem = pl.BlockSpec(memory_space=pltpu.VMEM)
    outs = pl.pallas_call(
        functools.partial(kernel, n, groups),
        out_shape=(
            jax.ShapeDtypeStruct((rows, width), bf16),
            jax.ShapeDtypeStruct((rows, width), bf16),
            jax.ShapeDtypeStruct((rows, model), bf16),
            jax.ShapeDtypeStruct((model // n, LANES), f32),
        ),
        in_specs=[vmem] * 7,
        out_specs=(vmem,) * 4,
        scratch_shapes=[
            pltpu.VMEM((groups, 4, n, rows, LANES), bf16),
            pltpu.VMEM((groups, 3, n, rows, LANES), bf16),
            pltpu.VMEM((8, rows, LANES), bf16),
            pltpu.VMEM((8, rows, LANES), bf16),
            pltpu.VMEM((8, rows, model), bf16),
            pltpu.VMEM((8, n, model // n, LANES), bf16),
            pltpu.VMEM((n, LANES, model // n), bf16),
            pltpu.VMEM((n - 1, LANES, model // n), bf16),
            pltpu.VMEM((LANES, padded), f32),
            pltpu.VMEM((padded, LANES), f32),
            pltpu.VMEM((length, LANES), f32),
            pltpu.VMEM((length, LANES), f32),
            pltpu.VMEM((length, LANES), f32),
            pltpu.SemaphoreType.DMA((copies,)),
            pltpu.SemaphoreType.DMA((copies,)),
        ],
        compiler_params=pltpu.CompilerParams(
            collective_id=0, has_side_effects=True, vmem_limit_bytes=60 * 2**20
        ),
    )(inputs[0], query[0], key[0], value[0], cotangent[0], gate[0], weight)
    query_grad, key_grad, input_grad, weight_grad = outs
    return (query_grad[None], key_grad[None], input_grad[None], weight_grad)


def solution(mesh):
    in_specs = (
        P("dp", "sp", None),
        P("dp", "sp", None),
        P("dp", "sp", None),
        P("dp", "sp", None),
        P("dp", "sp", None),
        P("dp", "sp", None),
        P("sp", "dp"),
    )
    out_specs = (P("dp", "sp", None), P("dp", "sp", None), P("dp", "sp", None), P("sp", "dp"))
    sp_count, dp_count = mesh.shape["sp"], mesh.shape["dp"]

    def per_device(*arrays):
        if one_kernel_fits(sp_count, dp_count, *arrays):
            return fused(mesh, *arrays)
        return shards(*arrays)

    return jax.shard_map(per_device, mesh=mesh, in_specs=in_specs, out_specs=out_specs, check_vma=False)
```

```python
import functools

import jax
import jax.numpy as jnp
from jax import lax
from jax.experimental import pallas as pl
from jax.experimental.pallas import tpu as pltpu
from jax.sharding import PartitionSpec as P

HEAD_DIM = 64


def attention_backward(query_heads, key_heads, value_heads, grad_heads, prefix):
    length = query_heads.shape[0]
    score_scale = HEAD_DIM ** (-0.5)
    block_count = max(1, length // 512)
    block_rows = length // block_count
    key_accum = jnp.zeros(key_heads.shape, jnp.float32)
    value_accum = jnp.zeros(key_heads.shape, jnp.float32)
    query_parts = []
    for block_index in range(block_count):
        first_row = block_index * block_rows
        last_row = first_row + block_rows
        query_rows = query_heads[first_row:last_row]
        key_rows = key_heads[:last_row]
        grad_rows = grad_heads[first_row:last_row]
        scores = (
            jnp.einsum("qhd,khd->hqk", query_rows, key_rows, preferred_element_type=jnp.float32)
            * score_scale
        )
        scores = scores + prefix[:, first_row:last_row, None] - prefix[:, None, :last_row]
        causal = jnp.arange(last_row)[None, :] <= (first_row + jnp.arange(block_rows))[:, None]
        scores = jnp.where(causal[None], scores, -jnp.inf)
        row_peak = jnp.max(scores, axis=-1, keepdims=True)
        raised_scores = jnp.exp(scores - row_peak)
        softmax_rows = raised_scores / jnp.sum(raised_scores, axis=-1, keepdims=True)
        softmax_low = softmax_rows.astype(jnp.bfloat16)
        value_accum = value_accum.at[:last_row].add(
            jnp.einsum("hqk,qhd->khd", softmax_low, grad_rows, preferred_element_type=jnp.float32)
        )
        softmax_grad = jnp.einsum(
            "qhd,khd->hqk", grad_rows, value_heads[:last_row], preferred_element_type=jnp.float32
        )
        row_term = jnp.sum(softmax_rows * softmax_grad, axis=-1, keepdims=True)
        score_low = (softmax_rows * (softmax_grad - row_term)).astype(jnp.bfloat16)
        query_parts.append(
            (
                jnp.einsum("hqk,khd->qhd", score_low, key_rows, preferred_element_type=jnp.float32)
                * score_scale
            ).astype(jnp.bfloat16)
        )
        key_accum = key_accum.at[:last_row].add(
            jnp.einsum("hqk,qhd->khd", score_low, query_rows, preferred_element_type=jnp.float32)
        )
    query_grad = jnp.concatenate(query_parts, axis=0)
    key_grad = (key_accum * score_scale).astype(jnp.bfloat16)
    return (query_grad, key_grad, value_accum.astype(jnp.bfloat16))


def shards(inputs, query_vectors, key_vectors, value_vectors, cotangent, gate_prefix, value_weight):
    query_seq, key_seq, value_seq, grad_seq, input_cols = (
        lax.all_to_all(query_vectors[0], "sp", split_axis=1, concat_axis=0, tiled=True),
        lax.all_to_all(key_vectors[0], "sp", split_axis=1, concat_axis=0, tiled=True),
        lax.all_to_all(value_vectors[0], "sp", split_axis=1, concat_axis=0, tiled=True),
        lax.all_to_all(cotangent[0], "sp", split_axis=1, concat_axis=0, tiled=True),
        lax.all_to_all(inputs[0], "sp", split_axis=1, concat_axis=0, tiled=True),
    )
    length = query_seq.shape[0]
    local_width = query_seq.shape[1]
    head_shape = (length, local_width // HEAD_DIM, HEAD_DIM)
    query_heads, key_heads, value_heads = attention_backward(
        query_seq.reshape(head_shape),
        key_seq.reshape(head_shape),
        value_seq.reshape(head_shape),
        grad_seq.reshape(head_shape),
        gate_prefix[0],
    )
    query_flat = query_heads.reshape(length, local_width)
    key_flat = key_heads.reshape(length, local_width)
    value_flat = value_heads.reshape(length, local_width)
    value_all = lax.all_gather(value_flat, "sp", axis=1, tiled=True)
    weight_block = lax.all_gather(value_weight, "dp", axis=1, tiled=True)
    weight_rows = lax.psum_scatter(
        lax.dot_general(
            value_all, input_cols, (((0,), (0,)), ((), ())), preferred_element_type=jnp.float32
        ).astype(jnp.bfloat16),
        "dp",
        scatter_dimension=0,
        tiled=True,
    ).astype(jnp.float32)
    weight_grad = weight_rows.T
    query_back, key_back = (
        lax.all_to_all(query_flat, "sp", split_axis=0, concat_axis=1, tiled=True),
        lax.all_to_all(key_flat, "sp", split_axis=0, concat_axis=1, tiled=True),
    )
    column_grad = lax.dot_general(
        value_all, weight_block, (((1,), (1,)), ((), ())), preferred_element_type=jnp.float32
    ).astype(jnp.bfloat16)
    input_grad = lax.all_to_all(column_grad, "sp", split_axis=0, concat_axis=1, tiled=True)
    return (query_back[None], key_back[None], input_grad[None], weight_grad)


LANES = 128
MESH = pl.DeviceIdType.MESH


def one_kernel_fits(sp_count, dp_count, inputs, query, key, value, cotangent, gate, weight):
    rows, width = query.shape[1:]
    model = inputs.shape[2]
    return (
        dp_count == 8
        and width == dp_count * LANES
        and width % (sp_count * LANES) == 0
        and LANES == 2 * HEAD_DIM
        and rows % 8 == 0
        and model % (sp_count * LANES) == 0
        and model % (2 * LANES) == 0
        and sp_count % 2 == 0
        and rows * sp_count <= 1024
        and (dp_count * rows + width) * model <= 3 * 2**21
    )


def query_blocks(length):
    return [(first, min(first + 256, length)) for first in range(0, length, 256)]


def own_lanes(head, *arrays):
    lane = lax.broadcasted_iota(jnp.int32, arrays[0].shape, 1)
    own = (lane < HEAD_DIM) if head == 0 else (lane >= HEAD_DIM)
    return [jnp.where(own, x, 0.0).astype(jnp.bfloat16) for x in arrays]


def add_block(ref, value, seen):
    if seen:
        ref[:seen] += value[:seen]
    if seen < value.shape[0]:
        ref[seen : value.shape[0]] = value[seen:]


dot = functools.partial(lax.dot_general, preferred_element_type=jnp.float32)
BY_LANES = (((1,), (1,)), ((), ()))
BY_ROWS = (((0,), (0,)), ((), ()))
PLAIN = (((1,), (0,)), ((), ()))


def softmax_pair(q32, k32, g32, gate_rows, gate_columns, soft_refs, dv_ref):
    length = q32.shape[0]
    scale = HEAD_DIM ** (-0.5)
    q_all = q32.astype(jnp.bfloat16)
    for head in range(2):
        k_own, g_own = own_lanes(head, k32, g32)
        for first, last in query_blocks(length):
            size = last - first
            scores = dot(k_own[:last], q_all[first:last], BY_LANES) * scale
            scores = scores + gate_rows[head][:, first:last] - gate_columns[head][:last]
            key_pos = lax.broadcasted_iota(jnp.int32, (last, size), 0)
            query_pos = lax.broadcasted_iota(jnp.int32, (last, size), 1) + first
            scores = jnp.where(key_pos <= query_pos, scores, -jnp.inf)
            peak = jnp.max(scores, axis=0, keepdims=True)
            raised = jnp.exp(scores - peak)
            soft = raised * (1.0 / jnp.sum(raised, axis=0, keepdims=True))
            soft_refs[head][:last, first:last] = soft
            add_block(
                dv_ref, dot(soft.astype(jnp.bfloat16), g_own[first:last], PLAIN),
                first if head == 0 else last,
            )


def gradient_pair(q32, k32, v32, g32, soft_refs, dq_ref, dk_ref):
    length = q32.shape[0]
    scale = HEAD_DIM ** (-0.5)
    g_all = g32.astype(jnp.bfloat16)
    for head in range(2):
        q_own, k_own, v_own = own_lanes(head, q32, k32, v32)
        for first, last in query_blocks(length):
            soft = soft_refs[head][:last, first:last]
            soft_grad = dot(v_own[:last], g_all[first:last], BY_LANES)
            row_term = jnp.sum(soft * soft_grad, axis=0, keepdims=True)
            score_low = (soft * (soft_grad - row_term)).astype(jnp.bfloat16)
            add_block(
                dk_ref, dot(score_low, q_own[first:last], PLAIN) * scale,
                first if head == 0 else last,
            )
            dq = dot(score_low, k_own[:last], BY_ROWS) * scale
            if head == 0:
                dq_ref[first:last] = dq
            else:
                dq_ref[first:last] += dq


def kernel(
    n, groups, in_hbm, q_hbm, k_hbm, v_hbm, g_hbm, gate_ref, w_hbm,
    qg_ref, kg_ref, ig_ref, wg_ref,
    in_ref, q_ref, k_ref, v_ref, g_ref, w_ref,
    pair_in, pair_out, vg, vg_seq, x_all, w_all, part, part_in, gate_pad, gate_t,
    soft, dq_ref, dk_ref, dv_ref, local_sems, hop_sems, hop_recv_sems, send_sems, recv_sems,
):
    s = lax.axis_index("sp")
    d = lax.axis_index("dp")
    core, x, y = d % 2, (d // 2) % 2, d // 4
    rows = q_ref.shape[0]
    length = n * rows
    half = in_ref.shape[1] // 2

    fetched = [
        pltpu.make_async_copy(src, dst, local_sems.at[i])
        for i, (src, dst) in enumerate(
            ((w_hbm, w_ref), (q_hbm, q_ref), (k_hbm, k_ref), (g_hbm, g_ref), (in_hbm, in_ref), (v_hbm, v_ref))
        )
    ]
    for copy in fetched:
        copy.start()

    def near(step):
        return (
            d
            + (step % 2) * (1 - 2 * core)
            + ((step // 2) % 2) * (2 - 4 * x)
            + (step // 4) * (4 - 8 * y)
        )

    partner, x_near, y_near, corner = near(1), near(2), near(4), near(6)
    started = []

    def send(src, dst, to_sp, to_dp):
        index = len(started)
        copy = pltpu.make_async_remote_copy(
            src_ref=src,
            dst_ref=dst,
            send_sem=send_sems.at[index],
            recv_sem=recv_sems.at[index],
            device_id={"sp": to_sp, "dp": to_dp},
            device_id_type=MESH,
        )
        copy.start()
        started.append(copy)
        return copy

    def lanes_of(device, p):
        return pl.ds(pl.multiple_of((device * groups + p) * LANES, LANES), LANES)

    barrier = pltpu.get_barrier_semaphore()
    for r in range(1, n):
        pl.semaphore_signal(barrier, inc=1, device_id={"sp": (s + r) % n, "dp": d}, device_id_type=MESH)
    for step in range(1, 8):
        pl.semaphore_signal(barrier, inc=1, device_id={"sp": s, "dp": near(step)}, device_id_type=MESH)
    pl.semaphore_wait(barrier, n - 1 + 7)
    for copy in fetched:
        copy.wait()

    def hop(t, up):
        block = (s - t + 1 + n) % n if up else (s + t - 1) % n
        src = w_ref if t == 1 else w_all.at[d, block]
        index = 2 * (t - 1) + int(up)
        return pltpu.make_async_remote_copy(
            src_ref=src,
            dst_ref=w_all.at[d, block],
            send_sem=hop_sems.at[index],
            recv_sem=hop_recv_sems.at[index],
            device_id={"sp": (s + 1) % n if up else (s - 1 + n) % n, "dp": d},
            device_id_type=MESH,
        )

    def hop_sends(t, act):
        pl.when((s >= t - 1) & (s < n - 1))(lambda: act(hop(t, True)))
        pl.when((s <= n - t) & (s > 0))(lambda: act(hop(t, False)))

    def hop_start(t):
        hop_sends(t, lambda copy: copy.start())

    def hop_arrive(t):
        pl.when(s >= t)(lambda: hop(t, True).wait_recv())
        pl.when(s < n - t)(lambda: hop(t, False).wait_recv())

    def send_pair(p, a, ref):
        return [
            send(ref.at[:, lanes_of((s + r) % n, p)], pair_in.at[p, a, s], (s + r) % n, d)
            for r in range(1, n)
        ]

    hop_start(1)
    early = [
        [c for a, ref in ((0, q_ref), (1, k_ref), (3, g_ref)) for c in send_pair(p, a, ref)]
        for p in range(groups)
    ]
    x_near0 = send(in_ref, x_all.at[d], s, x_near)
    y_near0 = send(in_ref, x_all.at[d], s, y_near)
    x_part0 = send(in_ref, x_all.at[d], s, partner)

    for p in range(groups):
        for a, ref in enumerate((q_ref, k_ref, v_ref, g_ref)):
            pair_in[p, a, s] = ref[:, lanes_of(s, p)]
    x_all[d] = in_ref[...]
    w_all[d, s] = w_ref[...]
    gate_pad[...] = jnp.zeros_like(gate_pad)
    gate_pad[: gate_ref.shape[0], :length] = gate_ref[...]
    gate_t[...] = gate_pad[...].T

    def wide(p, a):
        return pair_in[p, a].astype(jnp.float32).reshape(length, LANES)

    def give_back(p, a, ref):
        pair_out[p, a] = ref[...].reshape(n, rows, LANES).astype(jnp.bfloat16)
        copies = []
        for r in range(1, n):
            to = (s + r) % n
            dst = (
                vg.at[s * groups + p] if a == 0
                else (None, qg_ref, kg_ref)[a].at[:, lanes_of(s, p)]
            )
            copies.append(send(pair_out.at[p, a, to], dst, to, d))
        return copies

    def first_half(p):
        for copy in early[p]:
            copy.wait_recv()

    def softmax_part(p):
        heads = (2 * p, 2 * p + 1)
        softmax_pair(
            wide(p, 0), wide(p, 1), wide(p, 3),
            [gate_pad[h : h + 1, :length] for h in heads],
            [gate_t[:length, h : h + 1] for h in heads],
            [soft.at[h] for h in heads],
            dv_ref,
        )
        copies = give_back(p, 0, dv_ref)
        vg[s * groups + p] = pair_out[p, 0, s]
        return copies

    def gradient_part(p):
        gradient_pair(
            wide(p, 0), wide(p, 1), wide(p, 2), wide(p, 3),
            [soft.at[2 * p], soft.at[2 * p + 1]], dq_ref, dk_ref,
        )
        copies = give_back(p, 1, dq_ref) + give_back(p, 2, dk_ref)
        qg_ref[:, lanes_of(s, p)] = pair_out[p, 1, s]
        kg_ref[:, lanes_of(s, p)] = pair_out[p, 2, s]
        return copies

    def spread_middle(buffer, low, high, from_x, from_y):
        from_x.wait_recv()
        a = send(low(x_near), low(x_near), s, y_near)
        b = send(buffer.at[x_near], buffer.at[x_near], s, partner)
        from_y.wait_recv()
        c = send(high(y_near), high(y_near), s, x_near)
        e = send(buffer.at[y_near], buffer.at[y_near], s, partner)
        return a, c, b, e

    def spread_last(buffer, middle):
        middle[0].wait_recv()
        middle[1].wait_recv()
        return send(buffer.at[corner], buffer.at[corner], s, partner)

    x_low = lambda i: x_all.at[i, :, pl.ds(0, half)]
    x_high = lambda i: x_all.at[i, :, pl.ds(half, half)]
    w_low = lambda i: w_all.at[i, pl.ds(0, n // 2)]
    w_high = lambda i: w_all.at[i, pl.ds(n // 2, n // 2)]

    back_v, back_qk, late = [], [], []
    x_middle = None
    hop_next = 1

    def relay():
        nonlocal hop_next
        if hop_next < n:
            hop_arrive(hop_next)
            if hop_next + 1 < n:
                hop_start(hop_next + 1)
            hop_next += 1

    relay()
    for p in range(groups):
        first_half(p)
        if p == 0:
            late = [send_pair(i, 2, v_ref) for i in range(groups)]
        back_v += softmax_part(p)
        relay()
        if p == 0:
            x_middle = spread_middle(x_all, x_low, x_high, x_near0, y_near0)
    while hop_next < n:
        relay()
    w_x = send(w_all.at[d], w_all.at[d], s, x_near)
    w_y = send(w_all.at[d], w_all.at[d], s, y_near)
    w_part = send(w_all.at[d], w_all.at[d], s, partner)
    x_last = spread_last(x_all, x_middle)

    for copy in late[0]:
        copy.wait_recv()
    back_qk += gradient_part(0)

    for copy in back_v:
        copy.wait_recv()
    moved = [send(vg.at[near(step)], vg_seq.at[d], s, near(step)) for step in range(1, 8)]
    vg_seq[d] = vg[d]
    for p in range(1, groups):
        for copy in late[p]:
            copy.wait_recv()
        back_qk += gradient_part(p)
    w_middle = spread_middle(w_all, w_low, w_high, w_x, w_y)
    for copy in (x_part0, x_middle[2], x_middle[3], x_last):
        copy.wait_recv()
    for copy in moved:
        copy.wait_recv()

    block = in_ref.shape[1] // n
    for j in range(n):
        total = None
        for i in range(8):
            term = dot(vg_seq[i], x_all[i, :, j * block : (j + 1) * block], BY_ROWS)
            total = term if total is None else total + term
        part[j] = total.astype(jnp.bfloat16)
    sums = [send(part.at[(s + r) % n], part_in.at[r - 1], (s + r) % n, d) for r in range(1, n)]

    w_last = spread_last(w_all, w_middle)
    for copy in (w_part, w_middle[2], w_middle[3], w_last):
        copy.wait_recv()
    vg_rows = jnp.concatenate([vg[i] for i in range(8)], axis=1)
    for j in range(n):
        w_rows = jnp.concatenate([w_all[i, j] for i in range(8)], axis=1)
        ig_ref[:, j * block : (j + 1) * block] = dot(vg_rows, w_rows, BY_LANES).astype(jnp.bfloat16)

    total = part[s].astype(jnp.float32)
    for r, copy in enumerate(sums):
        copy.wait_recv()
        total = total + part_in[r].astype(jnp.float32)
    wg_ref[...] = total.T
    for copy in back_qk:
        copy.wait_recv()
    for copy in started:
        copy.wait_send()
    for t in range(1, n):
        hop_sends(t, lambda copy: copy.wait_send())


def fused(mesh, inputs, query, key, value, cotangent, gate, weight):
    n = mesh.shape["sp"]
    rows, width = query.shape[1:]
    model = inputs.shape[2]
    groups = width // (n * LANES)
    length = n * rows
    padded = -(-length // LANES) * LANES
    bf16, f32 = jnp.bfloat16, jnp.float32
    copies = (n - 1) * (7 * groups + 1) + 2 * 8 + 7
    vmem = pl.BlockSpec(memory_space=pltpu.VMEM)
    hbm = pl.BlockSpec(memory_space=pl.ANY)
    outs = pl.pallas_call(
        functools.partial(kernel, n, groups),
        out_shape=(
            jax.ShapeDtypeStruct((rows, width), bf16),
            jax.ShapeDtypeStruct((rows, width), bf16),
            jax.ShapeDtypeStruct((rows, model), bf16),
            jax.ShapeDtypeStruct((model // n, LANES), f32),
        ),
        in_specs=[hbm] * 5 + [vmem, hbm],
        out_specs=(vmem,) * 4,
        scratch_shapes=[
            pltpu.VMEM((rows, model), bf16),
            *[pltpu.VMEM((rows, width), bf16)] * 4,
            pltpu.VMEM((model // n, LANES), bf16),
            pltpu.VMEM((groups, 4, n, rows, LANES), bf16),
            pltpu.VMEM((groups, 3, n, rows, LANES), bf16),
            pltpu.VMEM((8, rows, LANES), bf16),
            pltpu.VMEM((8, rows, LANES), bf16),
            pltpu.VMEM((8, rows, model), bf16),
            pltpu.VMEM((8, n, model // n, LANES), bf16),
            pltpu.VMEM((n, LANES, model // n), bf16),
            pltpu.VMEM((n - 1, LANES, model // n), bf16),
            pltpu.VMEM((LANES, padded), f32),
            pltpu.VMEM((padded, LANES), f32),
            pltpu.VMEM((2 * groups, length, length), f32),
            *[pltpu.VMEM((length, LANES), f32)] * 3,
            pltpu.SemaphoreType.DMA((6,)),
            *[pltpu.SemaphoreType.DMA((2 * (n - 1),))] * 2,
            pltpu.SemaphoreType.DMA((copies,)),
            pltpu.SemaphoreType.DMA((copies,)),
        ],
        compiler_params=pltpu.CompilerParams(
            collective_id=0, has_side_effects=True, vmem_limit_bytes=60 * 2**20
        ),
    )(inputs[0], query[0], key[0], value[0], cotangent[0], gate[0], weight)
    query_grad, key_grad, input_grad, weight_grad = outs
    return (query_grad[None], key_grad[None], input_grad[None], weight_grad)


def solution(mesh):
    in_specs = (
        P("dp", "sp", None),
        P("dp", "sp", None),
        P("dp", "sp", None),
        P("dp", "sp", None),
        P("dp", "sp", None),
        P("dp", "sp", None),
        P("sp", "dp"),
    )
    out_specs = (P("dp", "sp", None), P("dp", "sp", None), P("dp", "sp", None), P("sp", "dp"))
    sp_count, dp_count = mesh.shape["sp"], mesh.shape["dp"]

    def per_device(*arrays):
        if one_kernel_fits(sp_count, dp_count, *arrays):
            return fused(mesh, *arrays)
        return shards(*arrays)

    return jax.shard_map(per_device, mesh=mesh, in_specs=in_specs, out_specs=out_specs, check_vma=False)
```

```python
import functools

import jax
import jax.numpy as jnp
from jax import lax
from jax.experimental import pallas as pl
from jax.experimental.pallas import tpu as pltpu
from jax.sharding import PartitionSpec as P

HEAD_DIM = 64


def attention_backward(query_heads, key_heads, value_heads, grad_heads, prefix):
    length = query_heads.shape[0]
    score_scale = HEAD_DIM ** (-0.5)
    block_count = max(1, length // 512)
    block_rows = length // block_count
    key_accum = jnp.zeros(key_heads.shape, jnp.float32)
    value_accum = jnp.zeros(key_heads.shape, jnp.float32)
    query_parts = []
    for block_index in range(block_count):
        first_row = block_index * block_rows
        last_row = first_row + block_rows
        query_rows = query_heads[first_row:last_row]
        key_rows = key_heads[:last_row]
        grad_rows = grad_heads[first_row:last_row]
        scores = (
            jnp.einsum("qhd,khd->hqk", query_rows, key_rows, preferred_element_type=jnp.float32)
            * score_scale
        )
        scores = scores + prefix[:, first_row:last_row, None] - prefix[:, None, :last_row]
        causal = jnp.arange(last_row)[None, :] <= (first_row + jnp.arange(block_rows))[:, None]
        scores = jnp.where(causal[None], scores, -jnp.inf)
        row_peak = jnp.max(scores, axis=-1, keepdims=True)
        raised_scores = jnp.exp(scores - row_peak)
        softmax_rows = raised_scores / jnp.sum(raised_scores, axis=-1, keepdims=True)
        softmax_low = softmax_rows.astype(jnp.bfloat16)
        value_accum = value_accum.at[:last_row].add(
            jnp.einsum("hqk,qhd->khd", softmax_low, grad_rows, preferred_element_type=jnp.float32)
        )
        softmax_grad = jnp.einsum(
            "qhd,khd->hqk", grad_rows, value_heads[:last_row], preferred_element_type=jnp.float32
        )
        row_term = jnp.sum(softmax_rows * softmax_grad, axis=-1, keepdims=True)
        score_low = (softmax_rows * (softmax_grad - row_term)).astype(jnp.bfloat16)
        query_parts.append(
            (
                jnp.einsum("hqk,khd->qhd", score_low, key_rows, preferred_element_type=jnp.float32)
                * score_scale
            ).astype(jnp.bfloat16)
        )
        key_accum = key_accum.at[:last_row].add(
            jnp.einsum("hqk,qhd->khd", score_low, query_rows, preferred_element_type=jnp.float32)
        )
    query_grad = jnp.concatenate(query_parts, axis=0)
    key_grad = (key_accum * score_scale).astype(jnp.bfloat16)
    return (query_grad, key_grad, value_accum.astype(jnp.bfloat16))


def shards(inputs, query_vectors, key_vectors, value_vectors, cotangent, gate_prefix, value_weight):
    query_seq, key_seq, value_seq, grad_seq, input_cols = (
        lax.all_to_all(query_vectors[0], "sp", split_axis=1, concat_axis=0, tiled=True),
        lax.all_to_all(key_vectors[0], "sp", split_axis=1, concat_axis=0, tiled=True),
        lax.all_to_all(value_vectors[0], "sp", split_axis=1, concat_axis=0, tiled=True),
        lax.all_to_all(cotangent[0], "sp", split_axis=1, concat_axis=0, tiled=True),
        lax.all_to_all(inputs[0], "sp", split_axis=1, concat_axis=0, tiled=True),
    )
    length = query_seq.shape[0]
    local_width = query_seq.shape[1]
    head_shape = (length, local_width // HEAD_DIM, HEAD_DIM)
    query_heads, key_heads, value_heads = attention_backward(
        query_seq.reshape(head_shape),
        key_seq.reshape(head_shape),
        value_seq.reshape(head_shape),
        grad_seq.reshape(head_shape),
        gate_prefix[0],
    )
    query_flat = query_heads.reshape(length, local_width)
    key_flat = key_heads.reshape(length, local_width)
    value_flat = value_heads.reshape(length, local_width)
    value_all = lax.all_gather(value_flat, "sp", axis=1, tiled=True)
    weight_block = lax.all_gather(value_weight, "dp", axis=1, tiled=True)
    weight_rows = lax.psum_scatter(
        lax.dot_general(
            value_all, input_cols, (((0,), (0,)), ((), ())), preferred_element_type=jnp.float32
        ).astype(jnp.bfloat16),
        "dp",
        scatter_dimension=0,
        tiled=True,
    ).astype(jnp.float32)
    weight_grad = weight_rows.T
    query_back, key_back = (
        lax.all_to_all(query_flat, "sp", split_axis=0, concat_axis=1, tiled=True),
        lax.all_to_all(key_flat, "sp", split_axis=0, concat_axis=1, tiled=True),
    )
    column_grad = lax.dot_general(
        value_all, weight_block, (((1,), (1,)), ((), ())), preferred_element_type=jnp.float32
    ).astype(jnp.bfloat16)
    input_grad = lax.all_to_all(column_grad, "sp", split_axis=0, concat_axis=1, tiled=True)
    return (query_back[None], key_back[None], input_grad[None], weight_grad)


LANES = 128
MESH = pl.DeviceIdType.MESH


def one_kernel_fits(sp_count, dp_count, inputs, query, key, value, cotangent, gate, weight):
    rows, width = query.shape[1:]
    model = inputs.shape[2]
    return (
        dp_count == 8
        and width == dp_count * LANES
        and width % (sp_count * LANES) == 0
        and LANES == 2 * HEAD_DIM
        and rows % 8 == 0
        and model % (sp_count * LANES) == 0
        and model % (2 * LANES) == 0
        and sp_count % 2 == 0
        and rows * sp_count <= 1024
        and (dp_count * rows + width) * model <= 3 * 2**21
    )


def query_blocks(length):
    return [(first, min(first + 256, length)) for first in range(0, length, 256)]


def own_lanes(head, *arrays):
    lane = lax.broadcasted_iota(jnp.int32, arrays[0].shape, 1)
    own = (lane < HEAD_DIM) if head == 0 else (lane >= HEAD_DIM)
    return [jnp.where(own, x, 0.0).astype(jnp.bfloat16) for x in arrays]


def add_block(ref, value, seen):
    if seen:
        ref[:seen] += value[:seen]
    if seen < value.shape[0]:
        ref[seen : value.shape[0]] = value[seen:]


dot = functools.partial(lax.dot_general, preferred_element_type=jnp.float32)
BY_LANES = (((1,), (1,)), ((), ()))
BY_ROWS = (((0,), (0,)), ((), ()))
PLAIN = (((1,), (0,)), ((), ()))


def softmax_pair(q32, k32, g32, gate_rows, gate_columns, soft_refs, dv_ref):
    length = q32.shape[0]
    scale = HEAD_DIM ** (-0.5)
    q_all = q32.astype(jnp.bfloat16)
    for head in range(2):
        k_own, g_own = own_lanes(head, k32, g32)
        for first, last in query_blocks(length):
            size = last - first
            scores = dot(k_own[:last], q_all[first:last], BY_LANES) * scale
            scores = scores + gate_rows[head][:, first:last] - gate_columns[head][:last]
            key_pos = lax.broadcasted_iota(jnp.int32, (last, size), 0)
            query_pos = lax.broadcasted_iota(jnp.int32, (last, size), 1) + first
            scores = jnp.where(key_pos <= query_pos, scores, -jnp.inf)
            peak = jnp.max(scores, axis=0, keepdims=True)
            raised = jnp.exp(scores - peak)
            soft = raised * (1.0 / jnp.sum(raised, axis=0, keepdims=True))
            soft_refs[head][:last, first:last] = soft
            add_block(
                dv_ref, dot(soft.astype(jnp.bfloat16), g_own[first:last], PLAIN),
                first if head == 0 else last,
            )


def gradient_pair(q32, k32, v32, g32, soft_refs, dq_ref, dk_ref):
    length = q32.shape[0]
    scale = HEAD_DIM ** (-0.5)
    g_all = g32.astype(jnp.bfloat16)
    for head in range(2):
        q_own, k_own, v_own = own_lanes(head, q32, k32, v32)
        for first, last in query_blocks(length):
            soft = soft_refs[head][:last, first:last]
            soft_grad = dot(v_own[:last], g_all[first:last], BY_LANES)
            row_term = jnp.sum(soft * soft_grad, axis=0, keepdims=True)
            score_low = (soft * (soft_grad - row_term)).astype(jnp.bfloat16)
            add_block(
                dk_ref, dot(score_low, q_own[first:last], PLAIN) * scale,
                first if head == 0 else last,
            )
            dq = dot(score_low, k_own[:last], BY_ROWS) * scale
            if head == 0:
                dq_ref[first:last] = dq
            else:
                dq_ref[first:last] += dq


def kernel(
    n, groups, in_hbm, q_hbm, k_hbm, v_hbm, g_hbm, gate_ref, w_hbm,
    qg_ref, kg_ref, ig_ref, wg_ref,
    in_ref, q_ref, k_ref, v_ref, g_ref, w_ref,
    pair_in, pair_out, vg, vg_seq, x_all, w_all, part, part_in, gate_pad, gate_t,
    soft, dq_ref, dk_ref, dv_ref, local_sems, hop_sems, hop_recv_sems, send_sems, recv_sems,
):
    s = lax.axis_index("sp")
    d = lax.axis_index("dp")
    core, x, y = d % 2, (d // 2) % 2, d // 4
    rows = q_ref.shape[0]
    length = n * rows
    half = in_ref.shape[1] // 2

    fetched = [
        pltpu.make_async_copy(src, dst, local_sems.at[i])
        for i, (src, dst) in enumerate(
            ((w_hbm, w_ref), (q_hbm, q_ref), (k_hbm, k_ref), (g_hbm, g_ref), (in_hbm, in_ref), (v_hbm, v_ref))
        )
    ]
    for copy in fetched:
        copy.start()

    def near(step):
        return (
            d
            + (step % 2) * (1 - 2 * core)
            + ((step // 2) % 2) * (2 - 4 * x)
            + (step // 4) * (4 - 8 * y)
        )

    partner, x_near, y_near, corner = near(1), near(2), near(4), near(6)
    started = []

    def send(src, dst, to_sp, to_dp):
        index = len(started)
        copy = pltpu.make_async_remote_copy(
            src_ref=src,
            dst_ref=dst,
            send_sem=send_sems.at[index],
            recv_sem=recv_sems.at[index],
            device_id={"sp": to_sp, "dp": to_dp},
            device_id_type=MESH,
        )
        copy.start()
        started.append(copy)
        return copy

    def lanes_of(device, p):
        return pl.ds(pl.multiple_of((device * groups + p) * LANES, LANES), LANES)

    barrier = pltpu.get_barrier_semaphore()
    for r in range(1, n):
        pl.semaphore_signal(barrier, inc=1, device_id={"sp": (s + r) % n, "dp": d}, device_id_type=MESH)
    for step in range(1, 8):
        pl.semaphore_signal(barrier, inc=1, device_id={"sp": s, "dp": near(step)}, device_id_type=MESH)
    pl.semaphore_wait(barrier, n - 1 + 7)
    for copy in fetched:
        copy.wait()

    def hop(t, up):
        block = (s - t + 1 + n) % n if up else (s + t - 1) % n
        src = w_ref if t == 1 else w_all.at[d, block]
        index = 2 * (t - 1) + int(up)
        return pltpu.make_async_remote_copy(
            src_ref=src,
            dst_ref=w_all.at[d, block],
            send_sem=hop_sems.at[index],
            recv_sem=hop_recv_sems.at[index],
            device_id={"sp": (s + 1) % n if up else (s - 1 + n) % n, "dp": d},
            device_id_type=MESH,
        )

    def hop_sends(t, act):
        pl.when((s >= t - 1) & (s < n - 1))(lambda: act(hop(t, True)))
        pl.when((s <= n - t) & (s > 0))(lambda: act(hop(t, False)))

    def hop_start(t):
        hop_sends(t, lambda copy: copy.start())

    def hop_arrive(t):
        pl.when(s >= t)(lambda: hop(t, True).wait_recv())
        pl.when(s < n - t)(lambda: hop(t, False).wait_recv())

    def send_pair(p, a, ref):
        return [
            send(ref.at[:, lanes_of((s + r) % n, p)], pair_in.at[p, a, s], (s + r) % n, d)
            for r in range(1, n)
        ]

    hop_start(1)
    early = [[] for _ in range(groups)]
    queue = [(p, a, ref) for p in range(groups) for a, ref in ((0, q_ref), (1, k_ref), (3, g_ref))]

    def send_early(count):
        for p, a, ref in queue[:count]:
            early[p].extend(send_pair(p, a, ref))
        del queue[:count]

    send_early(2)
    x_near0 = send(in_ref, x_all.at[d], s, x_near)
    y_near0 = send(in_ref, x_all.at[d], s, y_near)
    x_part0 = send(in_ref, x_all.at[d], s, partner)

    for p in range(groups):
        for a, ref in enumerate((q_ref, k_ref, v_ref, g_ref)):
            pair_in[p, a, s] = ref[:, lanes_of(s, p)]
    x_all[d] = in_ref[...]
    w_all[d, s] = w_ref[...]
    gate_pad[...] = jnp.zeros_like(gate_pad)
    gate_pad[: gate_ref.shape[0], :length] = gate_ref[...]
    gate_t[...] = gate_pad[...].T

    def wide(p, a):
        return pair_in[p, a].astype(jnp.float32).reshape(length, LANES)

    def give_back(p, a, ref):
        pair_out[p, a] = ref[...].reshape(n, rows, LANES).astype(jnp.bfloat16)
        copies = []
        for r in range(1, n):
            to = (s + r) % n
            dst = (
                vg.at[s * groups + p] if a == 0
                else (None, qg_ref, kg_ref)[a].at[:, lanes_of(s, p)]
            )
            copies.append(send(pair_out.at[p, a, to], dst, to, d))
        return copies

    def first_half(p):
        for copy in early[p]:
            copy.wait_recv()

    def softmax_part(p):
        heads = (2 * p, 2 * p + 1)
        softmax_pair(
            wide(p, 0), wide(p, 1), wide(p, 3),
            [gate_pad[h : h + 1, :length] for h in heads],
            [gate_t[:length, h : h + 1] for h in heads],
            [soft.at[h] for h in heads],
            dv_ref,
        )
        copies = give_back(p, 0, dv_ref)
        vg[s * groups + p] = pair_out[p, 0, s]
        return copies

    def gradient_part(p):
        gradient_pair(
            wide(p, 0), wide(p, 1), wide(p, 2), wide(p, 3),
            [soft.at[2 * p], soft.at[2 * p + 1]], dq_ref, dk_ref,
        )
        copies = give_back(p, 1, dq_ref) + give_back(p, 2, dk_ref)
        qg_ref[:, lanes_of(s, p)] = pair_out[p, 1, s]
        kg_ref[:, lanes_of(s, p)] = pair_out[p, 2, s]
        return copies

    def spread_middle(buffer, low, high, from_x, from_y):
        from_x.wait_recv()
        a = send(low(x_near), low(x_near), s, y_near)
        b = send(buffer.at[x_near], buffer.at[x_near], s, partner)
        from_y.wait_recv()
        c = send(high(y_near), high(y_near), s, x_near)
        e = send(buffer.at[y_near], buffer.at[y_near], s, partner)
        return a, c, b, e

    def spread_last(buffer, middle):
        middle[0].wait_recv()
        middle[1].wait_recv()
        return send(buffer.at[corner], buffer.at[corner], s, partner)

    x_low = lambda i: x_all.at[i, :, pl.ds(0, half)]
    x_high = lambda i: x_all.at[i, :, pl.ds(half, half)]
    w_low = lambda i: w_all.at[i, pl.ds(0, n // 2)]
    w_high = lambda i: w_all.at[i, pl.ds(n // 2, n // 2)]

    back_v, back_qk, late = [], [], []
    x_middle = None
    hop_next = 1

    def relay():
        nonlocal hop_next
        if hop_next < n:
            hop_arrive(hop_next)
            if hop_next + 1 < n:
                hop_start(hop_next + 1)
            hop_next += 1

    relay()
    send_early(2)
    relay()
    send_early(len(queue))
    x_middle = spread_middle(x_all, x_low, x_high, x_near0, y_near0)
    for p in range(groups):
        if p == groups - 1:
            while hop_next < n:
                relay()
            w_x = send(w_all.at[d], w_all.at[d], s, x_near)
            w_y = send(w_all.at[d], w_all.at[d], s, y_near)
            w_part = send(w_all.at[d], w_all.at[d], s, partner)
            x_last = spread_last(x_all, x_middle)
        first_half(p)
        back_v += softmax_part(p)
        late.append(send_pair(p, 2, v_ref))

    for p in range(groups - 1):
        for copy in late[p]:
            copy.wait_recv()
        back_qk += gradient_part(p)

    for copy in back_v:
        copy.wait_recv()
    moved = [send(vg.at[near(step)], vg_seq.at[d], s, near(step)) for step in range(1, 8)]
    vg_seq[d] = vg[d]
    w_middle = spread_middle(w_all, w_low, w_high, w_x, w_y)
    for copy in late[groups - 1]:
        copy.wait_recv()
    back_qk += gradient_part(groups - 1)
    for copy in (x_part0, x_middle[2], x_middle[3], x_last):
        copy.wait_recv()
    for copy in moved:
        copy.wait_recv()

    block = in_ref.shape[1] // n
    for j in range(n):
        total = None
        for i in range(8):
            term = dot(vg_seq[i], x_all[i, :, j * block : (j + 1) * block], BY_ROWS)
            total = term if total is None else total + term
        part[j] = total.astype(jnp.bfloat16)
    sums = [send(part.at[(s + r) % n], part_in.at[r - 1], (s + r) % n, d) for r in range(1, n)]

    w_last = spread_last(w_all, w_middle)
    for copy in (w_part, w_middle[2], w_middle[3], w_last):
        copy.wait_recv()
    vg_rows = jnp.concatenate([vg[i] for i in range(8)], axis=1)
    for j in range(n):
        w_rows = jnp.concatenate([w_all[i, j] for i in range(8)], axis=1)
        ig_ref[:, j * block : (j + 1) * block] = dot(vg_rows, w_rows, BY_LANES).astype(jnp.bfloat16)

    total = part[s].astype(jnp.float32)
    for r, copy in enumerate(sums):
        copy.wait_recv()
        total = total + part_in[r].astype(jnp.float32)
    wg_ref[...] = total.T
    for copy in back_qk:
        copy.wait_recv()
    for copy in started:
        copy.wait_send()
    for t in range(1, n):
        hop_sends(t, lambda copy: copy.wait_send())


def fused(mesh, inputs, query, key, value, cotangent, gate, weight):
    n = mesh.shape["sp"]
    rows, width = query.shape[1:]
    model = inputs.shape[2]
    groups = width // (n * LANES)
    length = n * rows
    padded = -(-length // LANES) * LANES
    bf16, f32 = jnp.bfloat16, jnp.float32
    copies = (n - 1) * (7 * groups + 1) + 2 * 8 + 7
    vmem = pl.BlockSpec(memory_space=pltpu.VMEM)
    hbm = pl.BlockSpec(memory_space=pl.ANY)
    results = (
        jax.ShapeDtypeStruct((rows, width), bf16),
        jax.ShapeDtypeStruct((rows, width), bf16),
        jax.ShapeDtypeStruct((rows, model), bf16),
        jax.ShapeDtypeStruct((model // n, LANES), f32),
    )
    outs = pl.pallas_call(
        functools.partial(kernel, n, groups),
        out_shape=tuple(pltpu.VMEM(x.shape, x.dtype) for x in results),
        in_specs=[hbm] * 5 + [vmem, hbm],
        out_specs=(vmem,) * 4,
        scratch_shapes=[
            pltpu.VMEM((rows, model), bf16),
            *[pltpu.VMEM((rows, width), bf16)] * 4,
            pltpu.VMEM((model // n, LANES), bf16),
            pltpu.VMEM((groups, 4, n, rows, LANES), bf16),
            pltpu.VMEM((groups, 3, n, rows, LANES), bf16),
            pltpu.VMEM((8, rows, LANES), bf16),
            pltpu.VMEM((8, rows, LANES), bf16),
            pltpu.VMEM((8, rows, model), bf16),
            pltpu.VMEM((8, n, model // n, LANES), bf16),
            pltpu.VMEM((n, LANES, model // n), bf16),
            pltpu.VMEM((n - 1, LANES, model // n), bf16),
            pltpu.VMEM((LANES, padded), f32),
            pltpu.VMEM((padded, LANES), f32),
            pltpu.VMEM((2 * groups, length, length), f32),
            *[pltpu.VMEM((length, LANES), f32)] * 3,
            pltpu.SemaphoreType.DMA((6,)),
            *[pltpu.SemaphoreType.DMA((2 * (n - 1),))] * 2,
            pltpu.SemaphoreType.DMA((copies,)),
            pltpu.SemaphoreType.DMA((copies,)),
        ],
        compiler_params=pltpu.CompilerParams(
            collective_id=0, has_side_effects=True, vmem_limit_bytes=60 * 2**20
        ),
    )(inputs[0], query[0], key[0], value[0], cotangent[0], gate[0], weight)
    query_grad, key_grad, input_grad, weight_grad = outs
    return (query_grad[None], key_grad[None], input_grad[None], weight_grad)


def solution(mesh):
    in_specs = (
        P("dp", "sp", None),
        P("dp", "sp", None),
        P("dp", "sp", None),
        P("dp", "sp", None),
        P("dp", "sp", None),
        P("dp", "sp", None),
        P("sp", "dp"),
    )
    out_specs = (P("dp", "sp", None), P("dp", "sp", None), P("dp", "sp", None), P("sp", "dp"))
    sp_count, dp_count = mesh.shape["sp"], mesh.shape["dp"]

    def per_device(*arrays):
        if one_kernel_fits(sp_count, dp_count, *arrays):
            return fused(mesh, *arrays)
        return shards(*arrays)

    return jax.shard_map(per_device, mesh=mesh, in_specs=in_specs, out_specs=out_specs, check_vma=False)
```

```python
import functools

import jax
import jax.numpy as jnp
from jax import lax
from jax.experimental import pallas as pl
from jax.experimental.pallas import tpu as pltpu
from jax.sharding import PartitionSpec as P

HEAD_DIM = 64


def attention_backward(query_heads, key_heads, value_heads, grad_heads, prefix):
    length = query_heads.shape[0]
    score_scale = HEAD_DIM ** (-0.5)
    block_count = max(1, length // 512)
    block_rows = length // block_count
    key_accum = jnp.zeros(key_heads.shape, jnp.float32)
    value_accum = jnp.zeros(key_heads.shape, jnp.float32)
    query_parts = []
    for block_index in range(block_count):
        first_row = block_index * block_rows
        last_row = first_row + block_rows
        query_rows = query_heads[first_row:last_row]
        key_rows = key_heads[:last_row]
        grad_rows = grad_heads[first_row:last_row]
        scores = (
            jnp.einsum("qhd,khd->hqk", query_rows, key_rows, preferred_element_type=jnp.float32)
            * score_scale
        )
        scores = scores + prefix[:, first_row:last_row, None] - prefix[:, None, :last_row]
        causal = jnp.arange(last_row)[None, :] <= (first_row + jnp.arange(block_rows))[:, None]
        scores = jnp.where(causal[None], scores, -jnp.inf)
        row_peak = jnp.max(scores, axis=-1, keepdims=True)
        raised_scores = jnp.exp(scores - row_peak)
        softmax_rows = raised_scores / jnp.sum(raised_scores, axis=-1, keepdims=True)
        softmax_low = softmax_rows.astype(jnp.bfloat16)
        value_accum = value_accum.at[:last_row].add(
            jnp.einsum("hqk,qhd->khd", softmax_low, grad_rows, preferred_element_type=jnp.float32)
        )
        softmax_grad = jnp.einsum(
            "qhd,khd->hqk", grad_rows, value_heads[:last_row], preferred_element_type=jnp.float32
        )
        row_term = jnp.sum(softmax_rows * softmax_grad, axis=-1, keepdims=True)
        score_low = (softmax_rows * (softmax_grad - row_term)).astype(jnp.bfloat16)
        query_parts.append(
            (
                jnp.einsum("hqk,khd->qhd", score_low, key_rows, preferred_element_type=jnp.float32)
                * score_scale
            ).astype(jnp.bfloat16)
        )
        key_accum = key_accum.at[:last_row].add(
            jnp.einsum("hqk,qhd->khd", score_low, query_rows, preferred_element_type=jnp.float32)
        )
    query_grad = jnp.concatenate(query_parts, axis=0)
    key_grad = (key_accum * score_scale).astype(jnp.bfloat16)
    return (query_grad, key_grad, value_accum.astype(jnp.bfloat16))


def shards(inputs, query_vectors, key_vectors, value_vectors, cotangent, gate_prefix, value_weight):
    query_seq, key_seq, value_seq, grad_seq, input_cols = (
        lax.all_to_all(query_vectors[0], "sp", split_axis=1, concat_axis=0, tiled=True),
        lax.all_to_all(key_vectors[0], "sp", split_axis=1, concat_axis=0, tiled=True),
        lax.all_to_all(value_vectors[0], "sp", split_axis=1, concat_axis=0, tiled=True),
        lax.all_to_all(cotangent[0], "sp", split_axis=1, concat_axis=0, tiled=True),
        lax.all_to_all(inputs[0], "sp", split_axis=1, concat_axis=0, tiled=True),
    )
    length = query_seq.shape[0]
    local_width = query_seq.shape[1]
    head_shape = (length, local_width // HEAD_DIM, HEAD_DIM)
    query_heads, key_heads, value_heads = attention_backward(
        query_seq.reshape(head_shape),
        key_seq.reshape(head_shape),
        value_seq.reshape(head_shape),
        grad_seq.reshape(head_shape),
        gate_prefix[0],
    )
    query_flat = query_heads.reshape(length, local_width)
    key_flat = key_heads.reshape(length, local_width)
    value_flat = value_heads.reshape(length, local_width)
    value_all = lax.all_gather(value_flat, "sp", axis=1, tiled=True)
    weight_block = lax.all_gather(value_weight, "dp", axis=1, tiled=True)
    weight_rows = lax.psum_scatter(
        lax.dot_general(
            value_all, input_cols, (((0,), (0,)), ((), ())), preferred_element_type=jnp.float32
        ).astype(jnp.bfloat16),
        "dp",
        scatter_dimension=0,
        tiled=True,
    ).astype(jnp.float32)
    weight_grad = weight_rows.T
    query_back, key_back = (
        lax.all_to_all(query_flat, "sp", split_axis=0, concat_axis=1, tiled=True),
        lax.all_to_all(key_flat, "sp", split_axis=0, concat_axis=1, tiled=True),
    )
    column_grad = lax.dot_general(
        value_all, weight_block, (((1,), (1,)), ((), ())), preferred_element_type=jnp.float32
    ).astype(jnp.bfloat16)
    input_grad = lax.all_to_all(column_grad, "sp", split_axis=0, concat_axis=1, tiled=True)
    return (query_back[None], key_back[None], input_grad[None], weight_grad)


LANES = 128
MESH = pl.DeviceIdType.MESH


def one_kernel_fits(sp_count, dp_count, inputs, query, key, value, cotangent, gate, weight):
    rows, width = query.shape[1:]
    model = inputs.shape[2]
    return (
        dp_count == 8
        and width == dp_count * LANES
        and width % (sp_count * LANES) == 0
        and LANES == 2 * HEAD_DIM
        and rows % 8 == 0
        and model % (sp_count * LANES) == 0
        and model % (2 * LANES) == 0
        and sp_count % 2 == 0
        and rows * sp_count <= 1024
        and (dp_count * rows + width) * model <= 3 * 2**21
    )


def query_blocks(length):
    return [(first, min(first + 256, length)) for first in range(0, length, 256)]


def own_lanes(head, *arrays):
    lane = lax.broadcasted_iota(jnp.int32, arrays[0].shape, 1)
    own = (lane < HEAD_DIM) if head == 0 else (lane >= HEAD_DIM)
    return [jnp.where(own, x, 0.0).astype(jnp.bfloat16) for x in arrays]


def add_block(ref, value, seen):
    if seen:
        ref[:seen] += value[:seen]
    if seen < value.shape[0]:
        ref[seen : value.shape[0]] = value[seen:]


dot = functools.partial(lax.dot_general, preferred_element_type=jnp.float32)
BY_LANES = (((1,), (1,)), ((), ()))
BY_ROWS = (((0,), (0,)), ((), ()))
PLAIN = (((1,), (0,)), ((), ()))


def softmax_pair(q32, k32, g32, gate_rows, gate_columns, soft_refs, dv_ref):
    length = q32.shape[0]
    scale = HEAD_DIM ** (-0.5)
    q_all = q32.astype(jnp.bfloat16)
    for head in range(2):
        k_own, g_own = own_lanes(head, k32, g32)
        for first, last in query_blocks(length):
            size = last - first
            scores = dot(k_own[:last], q_all[first:last], BY_LANES) * scale
            scores = scores + gate_rows[head][:, first:last] - gate_columns[head][:last]
            key_pos = lax.broadcasted_iota(jnp.int32, (last, size), 0)
            query_pos = lax.broadcasted_iota(jnp.int32, (last, size), 1) + first
            scores = jnp.where(key_pos <= query_pos, scores, -jnp.inf)
            peak = jnp.max(scores, axis=0, keepdims=True)
            raised = jnp.exp(scores - peak)
            soft = raised * (1.0 / jnp.sum(raised, axis=0, keepdims=True))
            soft_refs[head][:last, first:last] = soft
            add_block(
                dv_ref, dot(soft.astype(jnp.bfloat16), g_own[first:last], PLAIN),
                first if head == 0 else last,
            )


def gradient_pair(q32, k32, v32, g32, soft_refs, dq_ref, dk_ref):
    length = q32.shape[0]
    scale = HEAD_DIM ** (-0.5)
    g_all = g32.astype(jnp.bfloat16)
    for head in range(2):
        q_own, k_own, v_own = own_lanes(head, q32, k32, v32)
        for first, last in query_blocks(length):
            soft = soft_refs[head][:last, first:last]
            soft_grad = dot(v_own[:last], g_all[first:last], BY_LANES)
            row_term = jnp.sum(soft * soft_grad, axis=0, keepdims=True)
            score_low = (soft * (soft_grad - row_term)).astype(jnp.bfloat16)
            add_block(
                dk_ref, dot(score_low, q_own[first:last], PLAIN) * scale,
                first if head == 0 else last,
            )
            dq = dot(score_low, k_own[:last], BY_ROWS) * scale
            if head == 0:
                dq_ref[first:last] = dq
            else:
                dq_ref[first:last] += dq


def kernel(
    n, groups, in_hbm, q_hbm, k_hbm, v_hbm, g_hbm, gate_ref, w_hbm,
    qg_ref, kg_ref, ig_ref, wg_ref,
    in_ref, q_ref, k_ref, v_ref, g_ref, w_ref,
    pair_in, pair_out, vg, vg_seq, x_all, w_all, part, part_in, gate_pad, gate_t,
    soft, dq_ref, dk_ref, dv_ref, local_sems, hop_sems, hop_recv_sems, send_sems, recv_sems,
):
    s = lax.axis_index("sp")
    d = lax.axis_index("dp")
    core, x, y = d % 2, (d // 2) % 2, d // 4
    rows = q_ref.shape[0]
    length = n * rows
    half = in_ref.shape[1] // 2

    fetched = [
        pltpu.make_async_copy(src, dst, local_sems.at[i])
        for i, (src, dst) in enumerate(
            ((w_hbm, w_ref), (q_hbm, q_ref), (k_hbm, k_ref), (g_hbm, g_ref), (in_hbm, in_ref), (v_hbm, v_ref))
        )
    ]
    for copy in fetched:
        copy.start()

    def near(step):
        return (
            d
            + (step % 2) * (1 - 2 * core)
            + ((step // 2) % 2) * (2 - 4 * x)
            + (step // 4) * (4 - 8 * y)
        )

    partner, x_near, y_near, corner = near(1), near(2), near(4), near(6)
    started = []

    def send(src, dst, to_sp, to_dp):
        index = len(started)
        copy = pltpu.make_async_remote_copy(
            src_ref=src,
            dst_ref=dst,
            send_sem=send_sems.at[index],
            recv_sem=recv_sems.at[index],
            device_id={"sp": to_sp, "dp": to_dp},
            device_id_type=MESH,
        )
        copy.start()
        started.append(copy)
        return copy

    def lanes_of(device, p):
        return pl.ds(pl.multiple_of((device * groups + p) * LANES, LANES), LANES)

    barrier = pltpu.get_barrier_semaphore()
    for r in range(1, n):
        pl.semaphore_signal(barrier, inc=1, device_id={"sp": (s + r) % n, "dp": d}, device_id_type=MESH)
    for step in range(1, 8):
        pl.semaphore_signal(barrier, inc=1, device_id={"sp": s, "dp": near(step)}, device_id_type=MESH)
    pl.semaphore_wait(barrier, n - 1 + 7)
    for copy in fetched:
        copy.wait()

    def hop(t, up):
        block = (s - t + 1 + n) % n if up else (s + t - 1) % n
        src = w_ref if t == 1 else w_all.at[d, block]
        index = 2 * (t - 1) + int(up)
        return pltpu.make_async_remote_copy(
            src_ref=src,
            dst_ref=w_all.at[d, block],
            send_sem=hop_sems.at[index],
            recv_sem=hop_recv_sems.at[index],
            device_id={"sp": (s + 1) % n if up else (s - 1 + n) % n, "dp": d},
            device_id_type=MESH,
        )

    def hop_sends(t, act):
        pl.when((s >= t - 1) & (s < n - 1))(lambda: act(hop(t, True)))
        pl.when((s <= n - t) & (s > 0))(lambda: act(hop(t, False)))

    def hop_start(t):
        hop_sends(t, lambda copy: copy.start())

    def hop_arrive(t):
        pl.when(s >= t)(lambda: hop(t, True).wait_recv())
        pl.when(s < n - t)(lambda: hop(t, False).wait_recv())

    def send_pair(p, a, ref):
        return [
            send(ref.at[:, lanes_of((s + r) % n, p)], pair_in.at[p, a, s], (s + r) % n, d)
            for r in range(1, n)
        ]

    hop_start(1)
    early = [[] for _ in range(groups)]
    queue = [(p, a, ref) for p in range(groups) for a, ref in ((0, q_ref), (1, k_ref), (3, g_ref))]

    def send_early(count):
        for p, a, ref in queue[:count]:
            early[p].extend(send_pair(p, a, ref))
        del queue[:count]

    send_early(2)
    x_near0 = send(in_ref, x_all.at[d], s, x_near)
    y_near0 = send(in_ref, x_all.at[d], s, y_near)
    x_part0 = send(in_ref, x_all.at[d], s, partner)

    for p in range(groups):
        for a, ref in enumerate((q_ref, k_ref, v_ref, g_ref)):
            pair_in[p, a, s] = ref[:, lanes_of(s, p)]
    x_all[d] = in_ref[...]
    w_all[d, s] = w_ref[...]
    gate_pad[...] = jnp.zeros_like(gate_pad)
    gate_pad[: gate_ref.shape[0], :length] = gate_ref[...]
    gate_t[...] = gate_pad[...].T

    def wide(p, a):
        return pair_in[p, a].astype(jnp.float32).reshape(length, LANES)

    def give_back(p, a, ref):
        pair_out[p, a] = ref[...].reshape(n, rows, LANES).astype(jnp.bfloat16)
        copies = []
        for r in range(1, n):
            to = (s + r) % n
            dst = (
                vg.at[s * groups + p] if a == 0
                else (None, qg_ref, kg_ref)[a].at[:, lanes_of(s, p)]
            )
            copies.append(send(pair_out.at[p, a, to], dst, to, d))
        return copies

    def first_half(p):
        for copy in early[p]:
            copy.wait_recv()

    def softmax_part(p):
        heads = (2 * p, 2 * p + 1)
        softmax_pair(
            wide(p, 0), wide(p, 1), wide(p, 3),
            [gate_pad[h : h + 1, :length] for h in heads],
            [gate_t[:length, h : h + 1] for h in heads],
            [soft.at[h] for h in heads],
            dv_ref,
        )
        copies = give_back(p, 0, dv_ref)
        vg[s * groups + p] = pair_out[p, 0, s]
        return copies

    def gradient_part(p):
        gradient_pair(
            wide(p, 0), wide(p, 1), wide(p, 2), wide(p, 3),
            [soft.at[2 * p], soft.at[2 * p + 1]], dq_ref, dk_ref,
        )
        copies = give_back(p, 1, dq_ref) + give_back(p, 2, dk_ref)
        qg_ref[:, lanes_of(s, p)] = pair_out[p, 1, s]
        kg_ref[:, lanes_of(s, p)] = pair_out[p, 2, s]
        return copies

    def spread_middle(buffer, low, high, from_x, from_y):
        from_x.wait_recv()
        a = send(low(x_near), low(x_near), s, y_near)
        b = send(buffer.at[x_near], buffer.at[x_near], s, partner)
        from_y.wait_recv()
        c = send(high(y_near), high(y_near), s, x_near)
        e = send(buffer.at[y_near], buffer.at[y_near], s, partner)
        return a, c, b, e

    def spread_last(buffer, middle):
        middle[0].wait_recv()
        middle[1].wait_recv()
        return send(buffer.at[corner], buffer.at[corner], s, partner)

    x_low = lambda i: x_all.at[i, :, pl.ds(0, half)]
    x_high = lambda i: x_all.at[i, :, pl.ds(half, half)]
    w_low = lambda i: w_all.at[i, pl.ds(0, n // 2)]
    w_high = lambda i: w_all.at[i, pl.ds(n // 2, n // 2)]

    back_v, back_qk, late = [], [], []
    x_middle = None
    hop_next = 1

    def relay():
        nonlocal hop_next
        if hop_next < n:
            hop_arrive(hop_next)
            if hop_next + 1 < n:
                hop_start(hop_next + 1)
            hop_next += 1

    relay()
    send_early(2)
    relay()
    send_early(len(queue))
    x_middle = spread_middle(x_all, x_low, x_high, x_near0, y_near0)
    for p in range(groups):
        if p == groups - 1:
            while hop_next < n:
                relay()
            w_x = send(w_all.at[d], w_all.at[d], s, x_near)
            w_y = send(w_all.at[d], w_all.at[d], s, y_near)
            w_part = send(w_all.at[d], w_all.at[d], s, partner)
            x_last = spread_last(x_all, x_middle)
        first_half(p)
        back_v += softmax_part(p)
        late.append(send_pair(p, 2, v_ref))

    for p in range(groups - 1):
        for copy in late[p]:
            copy.wait_recv()
        back_qk += gradient_part(p)

    for copy in back_v:
        copy.wait_recv()
    moved = [send(vg.at[near(step)], vg_seq.at[d], s, near(step)) for step in range(1, 8)]
    vg_seq[d] = vg[d]
    w_middle = spread_middle(w_all, w_low, w_high, w_x, w_y)
    for copy in late[groups - 1]:
        copy.wait_recv()
    back_qk += gradient_part(groups - 1)
    for copy in (x_part0, x_middle[2], x_middle[3], x_last):
        copy.wait_recv()
    for copy in moved:
        copy.wait_recv()

    block = in_ref.shape[1] // n
    def weight_part(j):
        columns = pl.ds(pl.multiple_of(j * block, LANES), block)
        total = None
        for i in range(8):
            term = dot(vg_seq[i], x_all[i, :, columns], BY_ROWS)
            total = term if total is None else total + term
        return total

    def send_part(j, slot, to):
        return send(part.at[j], part_in.at[slot], to, d)

    two_steps = n == 4
    if two_steps:
        mate, across = s + 1 - 2 * (s % 2), (s + 2) % n
        far = (mate + 2) % n
        part[far] = weight_part(far).astype(jnp.bfloat16)
        far_sum = send_part(far, 0, mate)
        part[mate] = weight_part(mate).astype(jnp.bfloat16)
        sums = [send_part(mate, 1, mate)]
        across_sum = weight_part(across)
        own_sum = weight_part(s)
        w_last = spread_last(w_all, w_middle)
        far_sum.wait_recv()
        part[across] = (across_sum + part_in[0].astype(jnp.float32)).astype(jnp.bfloat16)
        sums.append(send_part(across, 2, across))
    else:
        sums = []
        for r in range(1, n):
            to = (s + r) % n
            part[to] = weight_part(to).astype(jnp.bfloat16)
            sums.append(send_part(to, r - 1, to))
        own_sum = weight_part(s)
        w_last = spread_last(w_all, w_middle)
    first_slot = int(two_steps)

    for copy in (w_part, w_middle[2], w_middle[3], w_last):
        copy.wait_recv()
    vg_rows = jnp.concatenate([vg[i] for i in range(8)], axis=1)
    for j in range(n):
        w_rows = jnp.concatenate([w_all[i, j] for i in range(8)], axis=1)
        ig_ref[:, j * block : (j + 1) * block] = dot(vg_rows, w_rows, BY_LANES).astype(jnp.bfloat16)

    for copy in back_qk:
        copy.wait_recv()
    for copy in started:
        if all(copy is not other for other in sums):
            copy.wait_send()
    for t in range(1, n):
        hop_sends(t, lambda copy: copy.wait_send())
    total = own_sum
    for r, copy in enumerate(sums):
        copy.wait_recv()
        total = total + part_in[first_slot + r].astype(jnp.float32)
    wg_ref[...] = total.T
    for copy in sums:
        copy.wait_send()


def fused(mesh, inputs, query, key, value, cotangent, gate, weight):
    n = mesh.shape["sp"]
    rows, width = query.shape[1:]
    model = inputs.shape[2]
    groups = width // (n * LANES)
    length = n * rows
    padded = -(-length // LANES) * LANES
    bf16, f32 = jnp.bfloat16, jnp.float32
    copies = (n - 1) * (7 * groups + 1) + 2 * 8 + 7
    vmem = pl.BlockSpec(memory_space=pltpu.VMEM)
    hbm = pl.BlockSpec(memory_space=pl.ANY)
    results = (
        jax.ShapeDtypeStruct((rows, width), bf16),
        jax.ShapeDtypeStruct((rows, width), bf16),
        jax.ShapeDtypeStruct((rows, model), bf16),
        jax.ShapeDtypeStruct((model // n, LANES), f32),
    )
    outs = pl.pallas_call(
        functools.partial(kernel, n, groups),
        out_shape=tuple(pltpu.VMEM(x.shape, x.dtype) for x in results),
        in_specs=[hbm] * 5 + [vmem, hbm],
        out_specs=(vmem,) * 4,
        scratch_shapes=[
            pltpu.VMEM((rows, model), bf16),
            *[pltpu.VMEM((rows, width), bf16)] * 4,
            pltpu.VMEM((model // n, LANES), bf16),
            pltpu.VMEM((groups, 4, n, rows, LANES), bf16),
            pltpu.VMEM((groups, 3, n, rows, LANES), bf16),
            pltpu.VMEM((8, rows, LANES), bf16),
            pltpu.VMEM((8, rows, LANES), bf16),
            pltpu.VMEM((8, rows, model), bf16),
            pltpu.VMEM((8, n, model // n, LANES), bf16),
            pltpu.VMEM((n, LANES, model // n), bf16),
            pltpu.VMEM((n - 1, LANES, model // n), bf16),
            pltpu.VMEM((LANES, padded), f32),
            pltpu.VMEM((padded, LANES), f32),
            pltpu.VMEM((2 * groups, length, length), f32),
            *[pltpu.VMEM((length, LANES), f32)] * 3,
            pltpu.SemaphoreType.DMA((6,)),
            *[pltpu.SemaphoreType.DMA((2 * (n - 1),))] * 2,
            pltpu.SemaphoreType.DMA((copies,)),
            pltpu.SemaphoreType.DMA((copies,)),
        ],
        compiler_params=pltpu.CompilerParams(
            collective_id=0, has_side_effects=True, vmem_limit_bytes=60 * 2**20
        ),
    )(inputs[0], query[0], key[0], value[0], cotangent[0], gate[0], weight)
    query_grad, key_grad, input_grad, weight_grad = outs
    return (query_grad[None], key_grad[None], input_grad[None], weight_grad)


def solution(mesh):
    in_specs = (
        P("dp", "sp", None),
        P("dp", "sp", None),
        P("dp", "sp", None),
        P("dp", "sp", None),
        P("dp", "sp", None),
        P("dp", "sp", None),
        P("sp", "dp"),
    )
    out_specs = (P("dp", "sp", None), P("dp", "sp", None), P("dp", "sp", None), P("sp", "dp"))
    sp_count, dp_count = mesh.shape["sp"], mesh.shape["dp"]

    def per_device(*arrays):
        if one_kernel_fits(sp_count, dp_count, *arrays):
            return fused(mesh, *arrays)
        return shards(*arrays)

    return jax.shard_map(per_device, mesh=mesh, in_specs=in_specs, out_specs=out_specs, check_vma=False)
```

```python
import functools

import jax
import jax.numpy as jnp
from jax import lax
from jax.experimental import pallas as pl
from jax.experimental.pallas import tpu as pltpu
from jax.sharding import PartitionSpec as P

HEAD_DIM = 64


def attention_backward(query_heads, key_heads, value_heads, grad_heads, prefix):
    length = query_heads.shape[0]
    score_scale = HEAD_DIM ** (-0.5)
    block_count = max(1, length // 512)
    block_rows = length // block_count
    key_accum = jnp.zeros(key_heads.shape, jnp.float32)
    value_accum = jnp.zeros(key_heads.shape, jnp.float32)
    query_parts = []
    for block_index in range(block_count):
        first_row = block_index * block_rows
        last_row = first_row + block_rows
        query_rows = query_heads[first_row:last_row]
        key_rows = key_heads[:last_row]
        grad_rows = grad_heads[first_row:last_row]
        scores = (
            jnp.einsum("qhd,khd->hqk", query_rows, key_rows, preferred_element_type=jnp.float32)
            * score_scale
        )
        scores = scores + prefix[:, first_row:last_row, None] - prefix[:, None, :last_row]
        causal = jnp.arange(last_row)[None, :] <= (first_row + jnp.arange(block_rows))[:, None]
        scores = jnp.where(causal[None], scores, -jnp.inf)
        row_peak = jnp.max(scores, axis=-1, keepdims=True)
        raised_scores = jnp.exp(scores - row_peak)
        softmax_rows = raised_scores / jnp.sum(raised_scores, axis=-1, keepdims=True)
        softmax_low = softmax_rows.astype(jnp.bfloat16)
        value_accum = value_accum.at[:last_row].add(
            jnp.einsum("hqk,qhd->khd", softmax_low, grad_rows, preferred_element_type=jnp.float32)
        )
        softmax_grad = jnp.einsum(
            "qhd,khd->hqk", grad_rows, value_heads[:last_row], preferred_element_type=jnp.float32
        )
        row_term = jnp.sum(softmax_rows * softmax_grad, axis=-1, keepdims=True)
        score_low = (softmax_rows * (softmax_grad - row_term)).astype(jnp.bfloat16)
        query_parts.append(
            (
                jnp.einsum("hqk,khd->qhd", score_low, key_rows, preferred_element_type=jnp.float32)
                * score_scale
            ).astype(jnp.bfloat16)
        )
        key_accum = key_accum.at[:last_row].add(
            jnp.einsum("hqk,qhd->khd", score_low, query_rows, preferred_element_type=jnp.float32)
        )
    query_grad = jnp.concatenate(query_parts, axis=0)
    key_grad = (key_accum * score_scale).astype(jnp.bfloat16)
    return (query_grad, key_grad, value_accum.astype(jnp.bfloat16))


def shards(inputs, query_vectors, key_vectors, value_vectors, cotangent, gate_prefix, value_weight):
    query_seq, key_seq, value_seq, grad_seq, input_cols = (
        lax.all_to_all(query_vectors[0], "sp", split_axis=1, concat_axis=0, tiled=True),
        lax.all_to_all(key_vectors[0], "sp", split_axis=1, concat_axis=0, tiled=True),
        lax.all_to_all(value_vectors[0], "sp", split_axis=1, concat_axis=0, tiled=True),
        lax.all_to_all(cotangent[0], "sp", split_axis=1, concat_axis=0, tiled=True),
        lax.all_to_all(inputs[0], "sp", split_axis=1, concat_axis=0, tiled=True),
    )
    length = query_seq.shape[0]
    local_width = query_seq.shape[1]
    head_shape = (length, local_width // HEAD_DIM, HEAD_DIM)
    query_heads, key_heads, value_heads = attention_backward(
        query_seq.reshape(head_shape),
        key_seq.reshape(head_shape),
        value_seq.reshape(head_shape),
        grad_seq.reshape(head_shape),
        gate_prefix[0],
    )
    query_flat = query_heads.reshape(length, local_width)
    key_flat = key_heads.reshape(length, local_width)
    value_flat = value_heads.reshape(length, local_width)
    value_all = lax.all_gather(value_flat, "sp", axis=1, tiled=True)
    weight_block = lax.all_gather(value_weight, "dp", axis=1, tiled=True)
    weight_rows = lax.psum_scatter(
        lax.dot_general(
            value_all, input_cols, (((0,), (0,)), ((), ())), preferred_element_type=jnp.float32
        ).astype(jnp.bfloat16),
        "dp",
        scatter_dimension=0,
        tiled=True,
    ).astype(jnp.float32)
    weight_grad = weight_rows.T
    query_back, key_back = (
        lax.all_to_all(query_flat, "sp", split_axis=0, concat_axis=1, tiled=True),
        lax.all_to_all(key_flat, "sp", split_axis=0, concat_axis=1, tiled=True),
    )
    column_grad = lax.dot_general(
        value_all, weight_block, (((1,), (1,)), ((), ())), preferred_element_type=jnp.float32
    ).astype(jnp.bfloat16)
    input_grad = lax.all_to_all(column_grad, "sp", split_axis=0, concat_axis=1, tiled=True)
    return (query_back[None], key_back[None], input_grad[None], weight_grad)


LANES = 128
MESH = pl.DeviceIdType.MESH


def one_kernel_fits(sp_count, dp_count, inputs, query, key, value, cotangent, gate, weight):
    rows, width = query.shape[1:]
    model = inputs.shape[2]
    return (
        dp_count == 8
        and width == dp_count * LANES
        and width % (sp_count * LANES) == 0
        and LANES == 2 * HEAD_DIM
        and rows % 8 == 0
        and model % (sp_count * LANES) == 0
        and model % (2 * LANES) == 0
        and sp_count % 2 == 0
        and rows * sp_count <= 1024
        and (dp_count * rows + width) * model <= 3 * 2**21
    )


def query_blocks(length):
    return [(first, min(first + 256, length)) for first in range(0, length, 256)]


def own_lanes(head, *arrays):
    lane = lax.broadcasted_iota(jnp.int32, arrays[0].shape, 1)
    own = (lane < HEAD_DIM) if head == 0 else (lane >= HEAD_DIM)
    return [jnp.where(own, x, 0.0).astype(jnp.bfloat16) for x in arrays]


def add_block(ref, value, seen):
    if seen:
        ref[:seen] += value[:seen]
    if seen < value.shape[0]:
        ref[seen : value.shape[0]] = value[seen:]


dot = functools.partial(lax.dot_general, preferred_element_type=jnp.float32)
BY_LANES = (((1,), (1,)), ((), ()))
BY_ROWS = (((0,), (0,)), ((), ()))
PLAIN = (((1,), (0,)), ((), ()))


def softmax_pair(q32, k32, g32, gate_rows, gate_columns, soft_refs, dv_ref):
    length = q32.shape[0]
    scale = HEAD_DIM ** (-0.5)
    q_all = q32.astype(jnp.bfloat16)
    for head in range(2):
        k_own, g_own = own_lanes(head, k32, g32)
        for first, last in query_blocks(length):
            size = last - first
            scores = dot(k_own[:last], q_all[first:last], BY_LANES) * scale
            scores = scores + gate_rows[head][:, first:last] - gate_columns[head][:last]
            key_pos = lax.broadcasted_iota(jnp.int32, (last, size), 0)
            query_pos = lax.broadcasted_iota(jnp.int32, (last, size), 1) + first
            scores = jnp.where(key_pos <= query_pos, scores, -jnp.inf)
            peak = jnp.max(scores, axis=0, keepdims=True)
            raised = jnp.exp(scores - peak)
            soft = raised * (1.0 / jnp.sum(raised, axis=0, keepdims=True))
            soft_refs[head][:last, first:last] = soft
            add_block(
                dv_ref, dot(soft.astype(jnp.bfloat16), g_own[first:last], PLAIN),
                first if head == 0 else last,
            )


def gradient_pair(q32, k32, v32, g32, soft_refs, dq_ref, dk_ref):
    length = q32.shape[0]
    scale = HEAD_DIM ** (-0.5)
    g_all = g32.astype(jnp.bfloat16)
    for head in range(2):
        q_own, k_own, v_own = own_lanes(head, q32, k32, v32)
        for first, last in query_blocks(length):
            soft = soft_refs[head][:last, first:last]
            soft_grad = dot(v_own[:last], g_all[first:last], BY_LANES)
            row_term = jnp.sum(soft * soft_grad, axis=0, keepdims=True)
            score_low = (soft * (soft_grad - row_term)).astype(jnp.bfloat16)
            add_block(
                dk_ref, dot(score_low, q_own[first:last], PLAIN) * scale,
                first if head == 0 else last,
            )
            dq = dot(score_low, k_own[:last], BY_ROWS) * scale
            if head == 0:
                dq_ref[first:last] = dq
            else:
                dq_ref[first:last] += dq


def kernel(
    n, groups, in_hbm, q_hbm, k_hbm, v_hbm, g_hbm, gate_ref, w_hbm,
    qg_ref, kg_ref, ig_ref, wg_ref,
    in_ref, q_ref, k_ref, v_ref, g_ref, w_ref,
    pair_in, pair_out, vg, vg_seq, x_all, w_all, part, part_in, gate_pad, gate_t,
    soft, dq_ref, dk_ref, dv_ref, local_sems, hop_sems, hop_recv_sems, send_sems, recv_sems,
):
    s = lax.axis_index("sp")
    d = lax.axis_index("dp")
    core, x, y = d % 2, (d // 2) % 2, d // 4
    rows = q_ref.shape[0]
    length = n * rows
    half = in_ref.shape[1] // 2

    fetched = [
        pltpu.make_async_copy(src, dst, local_sems.at[i])
        for i, (src, dst) in enumerate(
            ((w_hbm, w_ref), (q_hbm, q_ref), (k_hbm, k_ref), (g_hbm, g_ref), (in_hbm, in_ref), (v_hbm, v_ref))
        )
    ]
    for copy in fetched:
        copy.start()

    def near(step):
        return (
            d
            + (step % 2) * (1 - 2 * core)
            + ((step // 2) % 2) * (2 - 4 * x)
            + (step // 4) * (4 - 8 * y)
        )

    partner, x_near, y_near, corner = near(1), near(2), near(4), near(6)
    started = []

    def send(src, dst, to_sp, to_dp):
        index = len(started)
        copy = pltpu.make_async_remote_copy(
            src_ref=src,
            dst_ref=dst,
            send_sem=send_sems.at[index],
            recv_sem=recv_sems.at[index],
            device_id={"sp": to_sp, "dp": to_dp},
            device_id_type=MESH,
        )
        copy.start()
        started.append(copy)
        return copy

    def lanes_of(device, p):
        return pl.ds(pl.multiple_of((device * groups + p) * LANES, LANES), LANES)

    barrier = pltpu.get_barrier_semaphore()
    for r in range(1, n):
        pl.semaphore_signal(barrier, inc=1, device_id={"sp": (s + r) % n, "dp": d}, device_id_type=MESH)
    for step in range(1, 8):
        pl.semaphore_signal(barrier, inc=1, device_id={"sp": s, "dp": near(step)}, device_id_type=MESH)
    pl.semaphore_wait(barrier, n - 1 + 7)
    for copy in fetched:
        copy.wait()

    def hop(t, up):
        block = (s - t + 1 + n) % n if up else (s + t - 1) % n
        src = w_ref if t == 1 else w_all.at[d, block]
        index = 2 * (t - 1) + int(up)
        return pltpu.make_async_remote_copy(
            src_ref=src,
            dst_ref=w_all.at[d, block],
            send_sem=hop_sems.at[index],
            recv_sem=hop_recv_sems.at[index],
            device_id={"sp": (s + 1) % n if up else (s - 1 + n) % n, "dp": d},
            device_id_type=MESH,
        )

    def hop_sends(t, act):
        pl.when((s >= t - 1) & (s < n - 1))(lambda: act(hop(t, True)))
        pl.when((s <= n - t) & (s > 0))(lambda: act(hop(t, False)))

    def hop_start(t):
        hop_sends(t, lambda copy: copy.start())

    def hop_arrive(t):
        pl.when(s >= t)(lambda: hop(t, True).wait_recv())
        pl.when(s < n - t)(lambda: hop(t, False).wait_recv())

    def send_pair(p, a, ref):
        return [
            send(ref.at[:, lanes_of((s + r) % n, p)], pair_in.at[p, a, s], (s + r) % n, d)
            for r in range(1, n)
        ]

    hop_start(1)
    early = [[] for _ in range(groups)]
    queue = [(p, a, ref) for p in range(groups) for a, ref in ((0, q_ref), (1, k_ref), (3, g_ref))]

    def send_early(count):
        for p, a, ref in queue[:count]:
            early[p].extend(send_pair(p, a, ref))
        del queue[:count]

    send_early(2)
    x_near0 = send(in_ref, x_all.at[d], s, x_near)
    y_near0 = send(in_ref, x_all.at[d], s, y_near)
    x_part0 = send(in_ref, x_all.at[d], s, partner)

    for p in range(groups):
        for a, ref in enumerate((q_ref, k_ref, v_ref, g_ref)):
            pair_in[p, a, s] = ref[:, lanes_of(s, p)]
    x_all[d] = in_ref[...]
    w_all[d, s] = w_ref[...]
    gate_pad[...] = jnp.zeros_like(gate_pad)
    gate_pad[: gate_ref.shape[0], :length] = gate_ref[...]
    gate_t[...] = gate_pad[...].T

    def wide(p, a):
        return pair_in[p, a].astype(jnp.float32).reshape(length, LANES)

    def give_back(p, a, ref):
        pair_out[p, a] = ref[...].reshape(n, rows, LANES).astype(jnp.bfloat16)
        copies = []
        for r in range(1, n):
            to = (s + r) % n
            dst = (
                vg.at[s * groups + p] if a == 0
                else (None, qg_ref, kg_ref)[a].at[:, lanes_of(s, p)]
            )
            copies.append(send(pair_out.at[p, a, to], dst, to, d))
        return copies

    def first_half(p):
        for copy in early[p]:
            copy.wait_recv()

    def softmax_part(p):
        heads = (2 * p, 2 * p + 1)
        softmax_pair(
            wide(p, 0), wide(p, 1), wide(p, 3),
            [gate_pad[h : h + 1, :length] for h in heads],
            [gate_t[:length, h : h + 1] for h in heads],
            [soft.at[h] for h in heads],
            dv_ref,
        )
        copies = give_back(p, 0, dv_ref)
        vg[s * groups + p] = pair_out[p, 0, s]
        return copies

    def gradient_part(p):
        gradient_pair(
            wide(p, 0), wide(p, 1), wide(p, 2), wide(p, 3),
            [soft.at[2 * p], soft.at[2 * p + 1]], dq_ref, dk_ref,
        )
        copies = give_back(p, 1, dq_ref) + give_back(p, 2, dk_ref)
        qg_ref[:, lanes_of(s, p)] = pair_out[p, 1, s]
        kg_ref[:, lanes_of(s, p)] = pair_out[p, 2, s]
        return copies

    def spread_middle(buffer, low, high, from_x, from_y):
        from_x.wait_recv()
        a = send(low(x_near), low(x_near), s, y_near)
        b = send(buffer.at[x_near], buffer.at[x_near], s, partner)
        from_y.wait_recv()
        c = send(high(y_near), high(y_near), s, x_near)
        e = send(buffer.at[y_near], buffer.at[y_near], s, partner)
        return a, c, b, e

    def spread_last(buffer, middle):
        middle[0].wait_recv()
        middle[1].wait_recv()
        return send(buffer.at[corner], buffer.at[corner], s, partner)

    x_low = lambda i: x_all.at[i, :, pl.ds(0, half)]
    x_high = lambda i: x_all.at[i, :, pl.ds(half, half)]
    w_low = lambda i: w_all.at[i, pl.ds(0, n // 2)]
    w_high = lambda i: w_all.at[i, pl.ds(n // 2, n // 2)]

    back_v, back_qk, late = [], [], []
    x_middle = None
    hop_next = 1

    def relay():
        nonlocal hop_next
        if hop_next < n:
            hop_arrive(hop_next)
            if hop_next + 1 < n:
                hop_start(hop_next + 1)
            hop_next += 1

    relay()
    send_early(2)
    relay()
    send_early(len(queue))
    x_middle = spread_middle(x_all, x_low, x_high, x_near0, y_near0)
    for p in range(groups):
        if p == groups - 1:
            while hop_next < n:
                relay()
            w_x = send(w_all.at[d], w_all.at[d], s, x_near)
            w_y = send(w_all.at[d], w_all.at[d], s, y_near)
            w_part = send(w_all.at[d], w_all.at[d], s, partner)
            x_last = spread_last(x_all, x_middle)
        first_half(p)
        back_v += softmax_part(p)
        late.append(send_pair(p, 2, v_ref))

    for p in range(groups - 1):
        for copy in late[p]:
            copy.wait_recv()
        back_qk += gradient_part(p)

    for copy in back_v:
        copy.wait_recv()
    moved = [send(vg.at[near(step)], vg_seq.at[d], s, near(step)) for step in range(1, 8)]
    vg_seq[d] = vg[d]
    w_middle = spread_middle(w_all, w_low, w_high, w_x, w_y)
    for copy in late[groups - 1]:
        copy.wait_recv()
    back_qk += gradient_part(groups - 1)
    for copy in (x_part0, x_middle[2], x_middle[3], x_last):
        copy.wait_recv()
    for copy in moved:
        copy.wait_recv()

    block = in_ref.shape[1] // n
    def weight_part(j):
        columns = pl.ds(pl.multiple_of(j * block, LANES), block)
        total = None
        for i in range(8):
            term = dot(vg_seq[i], x_all[i, :, columns], BY_ROWS)
            total = term if total is None else total + term
        return total

    def send_part(j, slot, to):
        return send(part.at[j], part_in.at[slot], to, d)

    two_steps = n == 4
    if two_steps:
        mate, across = s + 1 - 2 * (s % 2), (s + 2) % n
        far = (mate + 2) % n
        part[far] = weight_part(far).astype(jnp.bfloat16)
        far_sum = send_part(far, 0, mate)
        part[mate] = weight_part(mate).astype(jnp.bfloat16)
        sums = [send_part(mate, 1, mate)]
        across_sum = weight_part(across)
        own_sum = weight_part(s)
        w_last = spread_last(w_all, w_middle)
        far_sum.wait_recv()
        part[across] = (across_sum + part_in[0].astype(jnp.float32)).astype(jnp.bfloat16)
        sums.append(send_part(across, 2, across))
    else:
        sums = []
        for r in range(1, n):
            to = (s + r) % n
            part[to] = weight_part(to).astype(jnp.bfloat16)
            sums.append(send_part(to, r - 1, to))
        own_sum = weight_part(s)
        w_last = spread_last(w_all, w_middle)
    first_slot = int(two_steps)

    for copy in (w_part, w_middle[2], w_middle[3], w_last):
        copy.wait_recv()
    vg_rows = jnp.concatenate([vg[i] for i in range(8)], axis=1)
    for j in range(n):
        w_rows = jnp.concatenate([w_all[i, j] for i in range(8)], axis=1)
        ig_ref[:, j * block : (j + 1) * block] = dot(vg_rows, w_rows, BY_LANES).astype(jnp.bfloat16)

    for copy in back_qk:
        copy.wait_recv()
    for copy in started:
        if all(copy is not other for other in sums):
            copy.wait_send()
    for t in range(1, n):
        hop_sends(t, lambda copy: copy.wait_send())
    total = own_sum
    for r, copy in enumerate(sums):
        copy.wait_recv()
        total = total + part_in[first_slot + r].astype(jnp.float32)
    wg_ref[...] = total.T
    for copy in sums:
        copy.wait_send()


def put_out(*refs):
    sems = refs[-1]
    copies = [pltpu.make_async_copy(refs[i], refs[4 + i], sems.at[i]) for i in range(4)]
    for copy in copies:
        copy.start()
    for copy in copies:
        copy.wait()


def fused(mesh, inputs, query, key, value, cotangent, gate, weight):
    n = mesh.shape["sp"]
    rows, width = query.shape[1:]
    model = inputs.shape[2]
    groups = width // (n * LANES)
    length = n * rows
    padded = -(-length // LANES) * LANES
    bf16, f32 = jnp.bfloat16, jnp.float32
    copies = (n - 1) * (7 * groups + 1) + 2 * 8 + 7
    vmem = pl.BlockSpec(memory_space=pltpu.VMEM)
    hbm = pl.BlockSpec(memory_space=pl.ANY)
    results = (
        jax.ShapeDtypeStruct((rows, width), bf16),
        jax.ShapeDtypeStruct((rows, width), bf16),
        jax.ShapeDtypeStruct((rows, model), bf16),
        jax.ShapeDtypeStruct((model // n, LANES), f32),
    )
    outs = pl.pallas_call(
        functools.partial(kernel, n, groups),
        out_shape=tuple(pltpu.VMEM(x.shape, x.dtype) for x in results),
        in_specs=[hbm] * 5 + [vmem, hbm],
        out_specs=(vmem,) * 4,
        scratch_shapes=[
            pltpu.VMEM((rows, model), bf16),
            *[pltpu.VMEM((rows, width), bf16)] * 4,
            pltpu.VMEM((model // n, LANES), bf16),
            pltpu.VMEM((groups, 4, n, rows, LANES), bf16),
            pltpu.VMEM((groups, 3, n, rows, LANES), bf16),
            pltpu.VMEM((8, rows, LANES), bf16),
            pltpu.VMEM((8, rows, LANES), bf16),
            pltpu.VMEM((8, rows, model), bf16),
            pltpu.VMEM((8, n, model // n, LANES), bf16),
            pltpu.VMEM((n, LANES, model // n), bf16),
            pltpu.VMEM((n - 1, LANES, model // n), bf16),
            pltpu.VMEM((LANES, padded), f32),
            pltpu.VMEM((padded, LANES), f32),
            pltpu.VMEM((2 * groups, length, length), f32),
            *[pltpu.VMEM((length, LANES), f32)] * 3,
            pltpu.SemaphoreType.DMA((6,)),
            *[pltpu.SemaphoreType.DMA((2 * (n - 1),))] * 2,
            pltpu.SemaphoreType.DMA((copies,)),
            pltpu.SemaphoreType.DMA((copies,)),
        ],
        compiler_params=pltpu.CompilerParams(
            collective_id=0, has_side_effects=True, vmem_limit_bytes=60 * 2**20
        ),
    )(inputs[0], query[0], key[0], value[0], cotangent[0], gate[0], weight)
    query_grad, key_grad, input_grad, weight_grad = pl.pallas_call(
        put_out,
        out_shape=results,
        in_specs=[vmem] * 4,
        out_specs=(hbm,) * 4,
        scratch_shapes=[pltpu.SemaphoreType.DMA((4,))],
        compiler_params=pltpu.CompilerParams(vmem_limit_bytes=2**20),
    )(*(pltpu.with_memory_space_constraint(x, pltpu.VMEM) for x in outs))
    return (query_grad[None], key_grad[None], input_grad[None], weight_grad)


def solution(mesh):
    in_specs = (
        P("dp", "sp", None),
        P("dp", "sp", None),
        P("dp", "sp", None),
        P("dp", "sp", None),
        P("dp", "sp", None),
        P("dp", "sp", None),
        P("sp", "dp"),
    )
    out_specs = (P("dp", "sp", None), P("dp", "sp", None), P("dp", "sp", None), P("sp", "dp"))
    sp_count, dp_count = mesh.shape["sp"], mesh.shape["dp"]

    def per_device(*arrays):
        if one_kernel_fits(sp_count, dp_count, *arrays):
            return fused(mesh, *arrays)
        return shards(*arrays)

    return jax.shard_map(per_device, mesh=mesh, in_specs=in_specs, out_specs=out_specs, check_vma=False)
```
